256 devices in a mesh: ep: 64 (over z, y, core), tp: 4 (over x).
Axes of the slice: x: 4, y: 4, z: 8, core: 2. Of those that a mesh axis runs over, the one named last changes fastest.
Arguments:
- tokens: bfloat16 [1024, 2048], P('ep'), may hold values from -6 to 6
- norm_gain: float32 [2048], replicated, may hold values from 0.1 to 1.9
- query_weight: bfloat16 [2048, 1024], P(None, 'tp'), may hold values from -0.21875 to 0.21875
- key_weight: bfloat16 [2048, 512], P(None, 'tp'), may hold values from -0.125 to 0.125
- value_weight: bfloat16 [2048, 512], P(None, 'tp'), may hold values from -0.125 to 0.125
- output_weight: bfloat16 [1024, 2048], P('tp'), may hold values from -0.1875 to 0.1875
- head_gain: float32 [128], replicated, may hold values from 0.1 to 1.9
- lambdas: float32 [8], P('tp'), may hold values from 0.3 to 0.8
- key_cache: bfloat16 [1024, 1024, 4, 128], P('ep', None, 'tp')
- value_cache: bfloat16 [1024, 1024, 4, 128], P('ep', None, 'tp'), may hold values from -6 to 6
- lengths: int32 [1024], P('ep'), may hold values from 128 to 1024, as said below
- ffn_gain: float32 [2048], replicated, may hold values from 0.1 to 1.9
- routes: int32 [1024, 4], P('ep'), may hold values from 0 to 63, all different within a row; in each aligned block of 16 rows (0 to 15, 16 to 31, ...) at most 2 rows name the same one
- route_weight: float32 [1024, 4], P('ep'), may hold values from 0.1 to 1
- expert_gate: bfloat16 [64, 2048, 1024], P('ep', None, 'tp'), may hold values from -0.125 to 0.125
- expert_up: bfloat16 [64, 2048, 1024], P('ep', None, 'tp'), may hold values from -0.125 to 0.125
- expert_down: bfloat16 [64, 1024, 2048], P('ep', 'tp'), may hold values from -0.1875 to 0.1875
- dense_gate: bfloat16 [2048, 2048], P('tp'), may hold values from -0.125 to 0.125
- dense_up: bfloat16 [2048, 2048], P('tp'), may hold values from -0.125 to 0.125
- dense_down: bfloat16 [2048, 2048], P('tp'), may hold values from -0.1875 to 0.1875
- gate_vector: float32 [2048], P('tp')
Outputs:
- layer_out: bfloat16 [1024, 2048], P('ep', 'tp')
The draws below stay inside these ranges and needn't reach their ends.
Inputs may be any that keep to these rules, and one draw needn't show every extreme that they name: `routes`: each row names 4 different experts. Among the rows of one index of ep no expert is named by more than 2 rows, a bound that some block reaches. `lengths`: some sequence has length 1024. Cached positions at or past a sequence's length are not read.
All inputs are finite; a program needn't handle non-finite values.
Results may differ from the reference program's by a relative error of at most 0.015.
The reference program's roundings to bfloat16 on the way count: a program that leaves them out, or rounds other values in their place, can miss the bound.
Values may be sent and summed in bfloat16 or wider, within the bound.
No kernel may reach another device: no remote copies, remote signals or barrier semaphores. Data moves between devices by JAX's collectives and lax.ppermute only.
A program may use at most 128 MiB of HBM per device.

```python
import math
import jax
import jax.numpy as jnp
import numpy as np
from jax import lax

D = 2048
HEADS = 8
KV_HEADS = 4
DQK = 64
DV = 128
FFE = 1024
FFD = 2048
TOPK = 4
SEQ_DEV = 16
CACHE = 1024
SEQS = 1024
EXPERTS = 64
CAP = 2
N_EP = 64
N_TP = 4


def draw_key_cache(key, part):
    normal_key = jax.random.fold_in(jax.random.fold_in(key, 11), 0)
    base_draw = jax.random.normal(normal_key, (SEQS, CACHE, KV_HEADS, 2 * DQK), jnp.float32)
    return base_draw.astype(jnp.bfloat16)


def draw_lengths(key, part):
    base_key, chosen_key = jax.random.split(jax.random.fold_in(key, 23))
    drawn = jax.random.randint(base_key, (SEQS,), CACHE // 8, CACHE + 1)
    chosen = jax.random.randint(chosen_key, (), 0, SEQS)
    return jnp.where(jnp.arange(SEQS) == chosen, CACHE, drawn).astype(jnp.int32)


def draw_gate_vector(key, part):
    inner_key = jax.random.fold_in(key, 37)
    rising = 1.0 + 3.0 * jnp.arange(FFD, dtype=jnp.float32) / FFD
    base_draw = jax.random.normal(inner_key, (FFD,), jnp.float32)
    return (base_draw * rising / math.sqrt(FFD)).astype(jnp.float32)


def with_spikes(entries, own_key, source, target, parts, factor):
    def block_of(position):
        return (jnp.arange(entries.shape[position]) // (entries.shape[position] // parts)).reshape((-1,) + (1,) * (entries.ndim - 1 - position))

    one_side = jax.random.permutation(own_key, parts)[block_of(target)]
    second = (block_of(target) + parts // 2) % parts
    return jnp.where((block_of(source) == one_side) | (block_of(source) == second), factor * entries, entries)


def levels(stream_key, dims, shards, smallest, top_value):
    level = 1.0
    for position, parts in shards:
        heights = jax.random.uniform(jax.random.fold_in(jax.random.fold_in(stream_key, 6), position), (parts,), jnp.float32, smallest / len(shards), top_value / len(shards))
        level = level * jnp.repeat(jnp.exp(heights), dims[position] // parts).reshape((-1,) + (1,) * (len(dims) - 1 - position))
    return level


def assign_block(own_key, own, number, rows, number_of, top, most, slope):
    ranking = jax.random.permutation(own_key, number_of)
    heavy_load, usual = shares(number_of, rows * top, most, slope, True), shares(number_of, rows * top, most, slope, False)
    places = jnp.arange(number_of)

    def named(sizes, rotation):
        used = int((sizes > 0).sum())
        fixed = max(1, used // 4)
        passed = fixed + (places - fixed + rotation * (used - fixed)) % max(1, number_of - fixed)
        return jnp.zeros((number_of,), jnp.int32).at[ranking[jnp.where(places < fixed, places, passed)]].set(jnp.asarray(sizes, jnp.int32))

    sizes = jnp.where(number % 4 == 0, named(heavy_load, number // 4), named(usual, number - number // 4 - 1))
    mixed = jax.random.permutation(jax.random.fold_in(own, 3), number_of)
    source_of, taker = mixed[0:number_of // 2 * 2:2], mixed[1:number_of // 2 * 2:2]
    room = jnp.minimum(sizes[source_of] - 1, most - sizes[taker]) // 2
    room = jnp.where((source_of == ranking[0]) | (taker == ranking[0]) | (sizes[taker] == 0), 0, jnp.maximum(room, 0))
    passed = jax.random.randint(jax.random.fold_in(own, 4), (number_of // 2,), 0, 1 << 20) % (room + 1)
    sizes = sizes.at[source_of].add(-passed).at[taker].add(passed)
    items = jnp.searchsorted(jnp.cumsum(sizes), jnp.arange(rows * top), side="right").astype(jnp.int32)
    listing = items.reshape(top, rows).T
    listing = listing[jax.random.permutation(jax.random.fold_in(own, 1), rows)]
    rotation = jax.random.randint(jax.random.fold_in(own, 2), (rows, 1), 0, top)
    return jnp.take_along_axis(listing, (jnp.arange(top)[None, :] + rotation) % top, axis=1)


def shares(count, total, bound, slope, full):
    loads = [(1 << 20) // math.isqrt(standing ** slope) + 1 for standing in range(1, count + 1)]
    largest = bound if full else min(bound, max(-(-total // count), total * loads[0] // sum(loads)))
    least = 1 if total - largest >= count - 1 else 0
    holding, surplus = [largest] + [least] * (count - 1), total - largest - least * (count - 1)
    while surplus > 0:
        candidates = [i for i in range(1, count) if holding[i] < largest] or [i for i in range(1, count) if holding[i] < bound]
        pool, left = sum([loads[i] for i in candidates]), surplus
        for i in candidates:
            addition = min(bound - holding[i], max(1, left * loads[i] // pool), surplus)
            holding[i] = holding[i] + addition
            surplus = surplus - addition
    return np.array(holding)


def gaussian(key, dims, width, reach, shards=(), held_as=jnp.bfloat16):
    values = jax.random.normal(key, dims, jnp.float32) * width
    if len(shards) > 0:
        values = levels(key, dims, shards, -0.22, 0.18) * values
    return jnp.clip(values, min=-reach, max=reach).astype(held_as)


def gaussian_with(stream_key, shape, width, limit, cuts, heavy, kind=jnp.bfloat16):
    values = width * jax.random.normal(stream_key, shape, jnp.float32)
    if cuts:
        values = values * levels(stream_key, shape, cuts, -0.22, 0.18)
    return jnp.clip(with_spikes(values, jax.random.fold_in(stream_key, 3), *heavy), -limit, limit).astype(kind)


def setup_inputs(seed: int = 0) -> dict:
    key_of = jax.random.split(jax.random.key(seed), 22)
    tokens = gaussian(key_of[0], (SEQS, D), 1.0, 6.0, ((0, 64),))
    norm_gain = jnp.clip(1.0 + 0.18 * jax.random.normal(key_of[1], (D,), jnp.float32), 0.1, 1.9)
    query_weight = gaussian(key_of[2], (D, HEADS * 2 * DQK), (D // 3) ** -0.5, 0.21875, ((1, 4),))
    key_weight = gaussian(key_of[3], (D, KV_HEADS * 2 * DQK), D ** -0.5, 0.125, ((1, 4),))
    value_weight = gaussian(key_of[4], (D, KV_HEADS * DV), D ** -0.5, 0.125, ((1, 4),))
    output_weight = gaussian(key_of[5], (HEADS * DV, D), (HEADS * DV) ** -0.5, 0.1875, ((0, 4),))
    head_gain = jnp.clip(1.0 + 0.18 * jax.random.normal(key_of[6], (DV,), jnp.float32), 0.1, 1.9)
    lambdas = jnp.clip(0.3 + 0.5 * jax.random.uniform(key_of[7], (HEADS,), jnp.float32) ** levels(key_of[7], (HEADS,), ((0, 4),), -0.2, 0.2), 0.3, 0.8)
    key_cache = draw_key_cache(jax.random.fold_in(key_of[21], 71), 0)
    value_cache = gaussian(key_of[9], (SEQS, CACHE, KV_HEADS, DV), 1.0, 6.0, ((0, 64), (2, 4)))
    lengths = draw_lengths(jax.random.fold_in(key_of[21], 71), 0)
    ffn_gain = jnp.clip(1.0 + 0.18 * jax.random.normal(key_of[11], (D,), jnp.float32), 0.1, 1.9)
    routes_keys = jax.random.split(jax.random.fold_in(key_of[12], 1), SEQS // SEQ_DEV)
    routes_turns = jax.random.permutation(jax.random.fold_in(key_of[12], 3), SEQS // SEQ_DEV)
    routes = jax.vmap(lambda own, number: assign_block(jax.random.fold_in(key_of[12], 2), own, number, SEQ_DEV, EXPERTS, TOPK, CAP, 2))(routes_keys, routes_turns).reshape((SEQS, TOPK))
    route_weight = jnp.clip(0.1 + 0.9 * jax.random.uniform(key_of[13], (SEQS, TOPK), jnp.float32) ** levels(key_of[13], (SEQS, TOPK), ((0, 64),), -0.2, 0.2), 0.1, 1.0)
    expert_gate = gaussian(key_of[14], (EXPERTS, D, FFE), D ** -0.5, 0.125, ((0, 64), (2, 4)))
    expert_up = gaussian(key_of[15], (EXPERTS, D, FFE), D ** -0.5, 0.125, ((0, 64), (2, 4)))
    expert_down = gaussian(key_of[16], (EXPERTS, FFE, D), FFE ** -0.5, 0.1875, ((0, 64), (1, 4)))
    dense_gate = gaussian(key_of[17], (FFD, D), D ** -0.5, 0.125, ((0, 4),))
    dense_up = gaussian(key_of[18], (FFD, D), D ** -0.5, 0.125, ((0, 4),))
    dense_down = gaussian_with(key_of[19], (FFD, D), FFD ** -0.5, 0.1875, ((0, 4),), (0, 1, 4, 2.0))
    gate_vector = draw_gate_vector(jax.random.fold_in(key_of[21], 71), 0)
    return {"tokens": tokens, "norm_gain": norm_gain, "query_weight": query_weight, "key_weight": key_weight, "value_weight": value_weight, "output_weight": output_weight, "head_gain": head_gain, "lambdas": lambdas, "key_cache": key_cache, "value_cache": value_cache, "lengths": lengths, "ffn_gain": ffn_gain, "routes": routes, "route_weight": route_weight, "expert_gate": expert_gate, "expert_up": expert_up, "expert_down": expert_down, "dense_gate": dense_gate, "dense_up": dense_up, "dense_down": dense_down, "gate_vector": gate_vector}


epsilon = 1e-06

def rms_scale(values, gain):
    return values * lax.rsqrt(lax.optimization_barrier(jnp.mean(values * values, axis=-1, keepdims=True)) + epsilon) * gain

def diff_attend(queries, new_key, new_value, key_rows, value_rows, length, lambda_grid):
    score_scale = DQK ** (-0.5)
    query_wide = queries.astype(jnp.float32)
    cache_scores = jnp.einsum('kgmd,ckmd->kgmc', query_wide, key_rows.astype(jnp.float32)) * score_scale
    own_score = jnp.einsum('kgmd,kmd->kgm', query_wide, new_key.astype(jnp.float32)) * score_scale
    live_mask = jnp.arange(CACHE) < length
    cache_scores = jnp.where(live_mask, cache_scores, -jnp.inf)
    top_score = jnp.maximum(lax.optimization_barrier(jnp.max(cache_scores, axis=-1)), own_score)
    cache_exp = jnp.exp(cache_scores - top_score[..., None])
    own_exp = jnp.exp(own_score - top_score)
    totals = lax.optimization_barrier(jnp.sum(cache_exp, axis=-1)) + own_exp
    cache_prob = cache_exp / totals[..., None]
    own_prob = own_exp / totals
    cache_weight = (cache_prob[:, :, 0] - lambda_grid[..., None] * cache_prob[:, :, 1]).astype(jnp.bfloat16)
    own_weight = (own_prob[:, :, 0] - lambda_grid * own_prob[:, :, 1]).astype(jnp.bfloat16)
    mixture = jnp.einsum('kgc,ckv->kgv', cache_weight.astype(jnp.float32), value_rows.astype(jnp.float32))
    return mixture + own_weight.astype(jnp.float32)[..., None] * new_value.astype(jnp.float32)[:, None, :]

def reference(tokens, norm_gain, query_weight, key_weight, value_weight, output_weight, head_gain, lambdas, key_cache, value_cache, lengths, ffn_gain, routes, route_weight, expert_gate, expert_up, expert_down, dense_gate, dense_up, dense_down, gate_vector):
    group_size = HEADS // KV_HEADS
    tokens_wide = tokens.astype(jnp.float32)
    normed = rms_scale(tokens_wide, norm_gain).astype(jnp.bfloat16)
    queries = jnp.dot(normed, query_weight, preferred_element_type=jnp.float32).astype(jnp.bfloat16)
    new_keys = jnp.dot(normed, key_weight, preferred_element_type=jnp.float32).astype(jnp.bfloat16)
    new_values = jnp.dot(normed, value_weight, preferred_element_type=jnp.float32).astype(jnp.bfloat16)
    queries = queries.reshape(SEQS, KV_HEADS, group_size, 2, DQK)
    new_keys = new_keys.reshape(SEQS, KV_HEADS, 2, DQK)
    new_values = new_values.reshape(SEQS, KV_HEADS, DV)
    lambda_grid = lambdas.reshape(KV_HEADS, group_size)

    def one_sequence(inputs):
        seq_query, seq_key, seq_value, seq_keys, seq_values, seq_length = inputs
        return diff_attend(seq_query, seq_key, seq_value, seq_keys.reshape(CACHE, KV_HEADS, 2, DQK), seq_values, seq_length, lambda_grid)
    mixture = lax.map(one_sequence, (queries, new_keys, new_values, key_cache, value_cache, lengths))
    head_rows = rms_scale(mixture, head_gain).astype(jnp.bfloat16).reshape(SEQS, HEADS * DV)
    block_rows = HEADS * DV // N_TP
    attention = jnp.zeros((SEQS, D), jnp.float32)
    for quarter in range(N_TP):
        partial_value = jnp.dot(head_rows[:, quarter * block_rows:(quarter + 1) * block_rows], output_weight[quarter * block_rows:(quarter + 1) * block_rows], preferred_element_type=jnp.float32)
        attention = attention + lax.optimization_barrier(partial_value.astype(jnp.bfloat16)).astype(jnp.float32)
    residual = tokens_wide + attention
    ffn_in = rms_scale(residual, ffn_gain).astype(jnp.bfloat16)
    gate_pre = jnp.dot(ffn_in, dense_gate.T, preferred_element_type=jnp.float32)
    up_proj = jnp.dot(ffn_in, dense_up.T, preferred_element_type=jnp.float32)
    dense_hidden = (jax.nn.silu(gate_pre) * up_proj).astype(jnp.bfloat16)
    gate_logit = lax.optimization_barrier(jnp.sum(dense_hidden.astype(jnp.float32) * gate_vector, axis=-1))
    dense_sum = jnp.dot(dense_hidden, dense_down, preferred_element_type=jnp.float32)
    dense_out = jax.nn.sigmoid(gate_logit)[:, None] * dense_sum
    pair_expert = routes.reshape(-1).astype(jnp.int32)
    onehot = (pair_expert[:, None] == jnp.arange(EXPERTS, dtype=jnp.int32)[None, :]).astype(jnp.int32)
    running = jnp.cumsum(onehot.reshape(N_EP, SEQ_DEV * TOPK, EXPERTS), axis=1).reshape(SEQS * TOPK, EXPERTS)
    slot_rank = lax.optimization_barrier(jnp.sum(running * onehot, axis=1)) - 1
    group_index = jnp.arange(SEQS * TOPK, dtype=jnp.int32) // (SEQ_DEV * TOPK)
    column = (group_index * CAP + slot_rank).astype(jnp.int32)
    token_of_pair = jnp.arange(SEQS * TOPK, dtype=jnp.int32) // TOPK
    buffer = jnp.zeros((EXPERTS, N_EP * CAP, D), jnp.bfloat16).at[pair_expert, column].set(ffn_in[token_of_pair])

    def expert_apply(inputs):
        row_block, w_gate, w_up, w_down = inputs
        expert_pre = jnp.dot(row_block, w_gate, preferred_element_type=jnp.float32)
        expert_upper = jnp.dot(row_block, w_up, preferred_element_type=jnp.float32)
        expert_hidden = (jax.nn.silu(expert_pre) * expert_upper).astype(jnp.bfloat16)
        quarter_width = FFE // N_TP
        summed = jnp.zeros((row_block.shape[0], D), jnp.float32)
        for quarter in range(N_TP):
            partial_value = jnp.dot(expert_hidden[:, quarter * quarter_width:(quarter + 1) * quarter_width], w_down[quarter * quarter_width:(quarter + 1) * quarter_width], preferred_element_type=jnp.float32)
            summed = summed + lax.optimization_barrier(partial_value.astype(jnp.bfloat16)).astype(jnp.float32)
        return summed.astype(jnp.bfloat16)
    expert_rows = lax.map(expert_apply, (buffer, expert_gate, expert_up, expert_down))
    picked = expert_rows[pair_expert, column].reshape(SEQS, TOPK, D).astype(jnp.float32)
    expert_mix = lax.optimization_barrier(jnp.sum(picked * route_weight[:, :, None], axis=1))
    return (residual + expert_mix + dense_out).astype(jnp.bfloat16)
```

```python
import jax
import jax.numpy as jnp
from jax import lax
from jax.experimental import pallas as pl
from jax.experimental.pallas import tpu as pltpu
from jax.sharding import PartitionSpec as P

HEADS = 8
KV_HEADS = 4
DQK = 64
DV = 128
TOPK = 4
CAP = 2
GROUP = 4

epsilon = 1e-06
F32 = jnp.float32
BF16 = jnp.bfloat16


def rms_scale(values, gain):
    return values * lax.rsqrt(jnp.mean(values * values, axis=-1, keepdims=True) + epsilon) * gain


def dot(lhs, rhs, contract=((1,), (0,))):
    return lax.dot_general(lhs, rhs, (contract, ((), ())), preferred_element_type=F32)


def attention_kernel(
    lengths,
    lambdas,
    tokens,
    norm_gain,
    head_gain,
    routes,
    route_weight,
    query_hbm,
    key_hbm,
    value_hbm,
    output_hbm,
    key_cache,
    value_cache,
    partial_out,
    dispatch_out,
    mix_out,
    query_weight,
    key_weight,
    value_weight,
    output_weight,
    keys,
    values,
    mixture,
    sems,
):
    seq_count = tokens.shape[0]
    groups = seq_count // GROUP
    copies = [
        pltpu.make_async_copy(query_hbm, query_weight, sems.at[0]),
        pltpu.make_async_copy(key_hbm, key_weight, sems.at[1]),
        pltpu.make_async_copy(value_hbm, value_weight, sems.at[2]),
    ]
    for group in range(groups):
        rows = pl.ds(group * GROUP, GROUP)
        copies.append(
            pltpu.make_async_copy(key_cache.at[rows], keys.at[rows], sems.at[4 + 2 * group])
        )
        copies.append(
            pltpu.make_async_copy(value_cache.at[rows], values.at[rows], sems.at[5 + 2 * group])
        )
    last = pltpu.make_async_copy(output_hbm, output_weight, sems.at[3])
    for copy in copies:
        copy.start()
    last.start()

    slots = dispatch_out.shape[0]
    slot_ids = lax.broadcasted_iota(jnp.int32, (slots, seq_count), 0)
    named = jnp.zeros((slots, seq_count), F32)
    weighed = jnp.zeros((slots, seq_count), F32)
    for k in range(TOPK):
        hit = (slot_ids // CAP) == routes[k : k + 1, :]
        named = named + jnp.where(hit, 1.0, 0.0)
        weighed = weighed + jnp.where(hit, route_weight[k : k + 1, :], 0.0)
    before = lax.broadcasted_iota(jnp.int32, (seq_count, seq_count), 0)
    after = lax.broadcasted_iota(jnp.int32, (seq_count, seq_count), 1)
    earlier = jnp.where(before < after, 1.0, 0.0).astype(BF16)
    rank = dot(named.astype(BF16), earlier)
    chosen = rank == (slot_ids % CAP).astype(F32)
    dispatch_out[...] = jnp.where(chosen, named, 0.0).astype(BF16)
    mix_out[...] = jnp.where(chosen, weighed, 0.0)

    normed = rms_scale(tokens[...].astype(F32), norm_gain[...]).astype(BF16)
    copies[0].wait()
    queries = dot(normed, query_weight[...]).astype(BF16).astype(F32)
    copies[1].wait()
    new_keys = dot(normed, key_weight[...]).astype(BF16).astype(F32)
    copies[2].wait()
    new_values = dot(normed, value_weight[...]).astype(BF16).astype(F32)

    cache_len = keys.shape[1]
    row = lax.broadcasted_iota(jnp.int32, (8, 2 * DQK), 0)
    lane = lax.broadcasted_iota(jnp.int32, (8, 2 * DQK), 1)
    keep = jnp.logical_and((lane // DQK) == (row % 2), row < 4)
    row1 = lax.broadcasted_iota(jnp.int32, (8, 1), 0)
    sign = jnp.where(row1 % 2 == 0, 1.0, -jnp.where(row1 < 2, lambdas[0], lambdas[1]))
    position = lax.broadcasted_iota(jnp.int32, (8, cache_len), 1)
    score_scale = DQK ** (-0.5)
    for group in range(groups):
        copies[3 + 2 * group].wait()
        scores = []
        own_scores = []
        for s in range(group * GROUP, (group + 1) * GROUP):
            first = jnp.broadcast_to(queries[s : s + 1, : 2 * DQK], (8, 2 * DQK))
            second = jnp.broadcast_to(queries[s : s + 1, 2 * DQK :], (8, 2 * DQK))
            query = jnp.where(keep, jnp.where(row < 2, first, second), 0.0)
            score = dot(query.astype(BF16), keys[s], ((1,), (1,))) * score_scale
            scores.append(jnp.where(position < lengths[s], score, -jnp.inf))
            own_scores.append(
                jnp.sum(query * new_keys[s : s + 1, :], axis=1, keepdims=True) * score_scale
            )
        weights = []
        own_weights = []
        for score, own in zip(scores, own_scores):
            top = jnp.maximum(jnp.max(score, axis=1, keepdims=True), own)
            grown = jnp.exp(score - top)
            own_grown = jnp.exp(own - top)
            total = jnp.sum(grown, axis=1, keepdims=True) + own_grown
            share = sign / total
            prob = grown * share
            own_prob = own_grown * share
            weights.append((prob + pltpu.roll(prob, 7, 0)).astype(BF16))
            own_weights.append((own_prob + pltpu.roll(own_prob, 7, 0)).astype(BF16).astype(F32))
        copies[4 + 2 * group].wait()
        for i in range(GROUP):
            s = group * GROUP + i
            mixed = dot(weights[i], values[s]) + own_weights[i] * new_values[s : s + 1, :]
            mixture[s : s + 1, :DV] = mixed[0:1, :]
            mixture[s : s + 1, DV:] = mixed[2:3, :]
    gain = head_gain[...]
    left = rms_scale(mixture[:, :DV], gain).astype(BF16)
    right = rms_scale(mixture[:, DV:], gain).astype(BF16)
    last.wait()
    result = dot(left, output_weight[:DV, :]) + dot(right, output_weight[DV:, :])
    partial_out[...] = result.astype(BF16)


def whole(count):
    return [pl.BlockSpec(memory_space=pltpu.VMEM)] * count


def attend(tokens, norm_gain, query_weight, key_weight, value_weight, output_weight, head_gain,
           lambdas, key_cache, value_cache, lengths, routes, route_weight, slots):
    seq_count, width = tokens.shape
    smem = pl.BlockSpec(memory_space=pltpu.SMEM)
    hbm = pl.BlockSpec(memory_space=pl.ANY)
    groups = seq_count // GROUP
    return pl.pallas_call(
        attention_kernel,
        name="attend",
        out_shape=(
            jax.ShapeDtypeStruct((seq_count, width), BF16),
            jax.ShapeDtypeStruct((slots, seq_count), BF16),
            jax.ShapeDtypeStruct((slots, seq_count), F32),
        ),
        in_specs=[smem, smem] + whole(5) + [hbm] * 6,
        out_specs=tuple(whole(3)),
        scratch_shapes=[
            pltpu.VMEM(query_weight.shape, BF16),
            pltpu.VMEM(key_weight.shape, BF16),
            pltpu.VMEM(value_weight.shape, BF16),
            pltpu.VMEM(output_weight.shape, BF16),
            pltpu.VMEM(key_cache.shape, BF16),
            pltpu.VMEM(value_cache.shape, BF16),
            pltpu.VMEM((seq_count, 2 * DV), F32),
            pltpu.SemaphoreType.DMA((4 + 2 * groups,)),
        ],
    )(lengths, lambdas, tokens, norm_gain, head_gain, routes, route_weight,
      query_weight, key_weight, value_weight, output_weight, key_cache, value_cache)


def normalise_kernel(tokens, own, one, two, three, gain, dispatch, residual, ffn_in, outbound):
    attention = (own[...].astype(F32) + one[...].astype(F32)) + (
        two[...].astype(F32) + three[...].astype(F32)
    )
    total = tokens[...].astype(F32) + attention
    residual[...] = total
    rows = rms_scale(total, gain[...]).astype(BF16)
    ffn_in[...] = rows
    outbound[...] = dot(dispatch[...], rows).astype(BF16)


def normalise(tokens, parts, gain, dispatch):
    seq_count, width = tokens.shape
    return pl.pallas_call(
        normalise_kernel,
        name="normalise",
        out_shape=(
            jax.ShapeDtypeStruct((seq_count, width), F32),
            jax.ShapeDtypeStruct((seq_count, width), BF16),
            jax.ShapeDtypeStruct((dispatch.shape[0], width), BF16),
        ),
        in_specs=whole(7),
        out_specs=tuple(whole(3)),
    )(tokens, *parts, gain, dispatch)


def silu(values):
    return values / (1.0 + jnp.exp(-values))


def dense_kernel(rows, gate, up, down, vector, term, logit):
    value = rows[...]
    gate_pre = dot(value, gate[...], ((1,), (1,)))
    up_proj = dot(value, up[...], ((1,), (1,)))
    hidden = (silu(gate_pre) * up_proj).astype(BF16)
    term[...] = dot(hidden, down[...]).astype(BF16)
    part = jnp.sum(hidden.astype(F32) * vector[...], axis=1, keepdims=True)
    high = part.astype(BF16)
    rest = part - high.astype(F32)
    middle = rest.astype(BF16)
    low = (rest - middle.astype(F32)).astype(BF16)
    lane = lax.broadcasted_iota(jnp.int32, logit.shape, 1)
    pieces = jnp.where(
        lane == 0, high.astype(F32), jnp.where(lane == 1, middle.astype(F32), low.astype(F32))
    )
    logit[...] = jnp.where(lane < 3, pieces, 0.0).astype(BF16)


def dense_branch(rows, gate, up, down, vector, columns):
    seq_count, width = rows.shape
    return pl.pallas_call(
        dense_kernel,
        name="dense",
        out_shape=(
            jax.ShapeDtypeStruct((seq_count, width), BF16),
            jax.ShapeDtypeStruct((seq_count, columns), BF16),
        ),
        in_specs=whole(5),
        out_specs=tuple(whole(2)),
        cost_estimate=pl.CostEstimate(
            flops=6 * seq_count * width * gate.shape[0],
            bytes_accessed=6 * width * gate.shape[0],
            transcendentals=0,
        ),
    )(rows, gate, up, down, vector)


def expert_kernel(place, rows, gate, up, down, term, logit, *blocks):
    value = rows[...]
    hidden = (silu(dot(value, gate[...])) * dot(value, up[...])).astype(BF16)
    count, columns = value.shape[0], blocks[0].shape[1]
    seq_count = term.shape[0]
    for step, block in enumerate(blocks):
        start = pl.multiple_of(((place[0] + step) % len(blocks)) * columns, columns)
        block[:count, :] = dot(hidden, down[:, pl.ds(start, columns)]).astype(BF16)
        block[count : count + seq_count, :] = term[:, pl.ds(start, columns)]
        block[count + seq_count :, :] = logit[...]


def expert_rows(place, rows, gate, up, down, term, logit, devices):
    count, width = rows.shape
    seq_count, columns = logit.shape
    shape = jax.ShapeDtypeStruct((count + 2 * seq_count, columns), BF16)
    return pl.pallas_call(
        expert_kernel,
        name="experts",
        out_shape=(shape,) * devices,
        in_specs=[pl.BlockSpec(memory_space=pltpu.SMEM)] + whole(6),
        out_specs=tuple(whole(devices)),
    )(place, rows, gate, up, down, term, logit)


def gather_kernel(place, own, one, two, three, residual, summed, kept):
    count, columns = summed.shape
    seq_count = residual.shape[0]
    total = (own[...].astype(F32) + one[...].astype(F32)) + (
        two[...].astype(F32) + three[...].astype(F32)
    )
    summed[...] = total[:count, :].astype(BF16)
    pieces = total[count + seq_count :, :]
    lane = lax.broadcasted_iota(jnp.int32, pieces.shape, 1)
    logit = jnp.sum(jnp.where(lane < 3, pieces, 0.0), axis=1, keepdims=True)
    gated = total[count : count + seq_count, :] / (1.0 + jnp.exp(-logit))
    start = pl.multiple_of(place[0] * columns, columns)
    kept[...] = residual[:, pl.ds(start, columns)] + gated


def gather_parts(place, parts, residual, count):
    seq_count = residual.shape[0]
    columns = parts[0].shape[1]
    return pl.pallas_call(
        gather_kernel,
        name="gather",
        out_shape=(
            jax.ShapeDtypeStruct((count, columns), BF16),
            jax.ShapeDtypeStruct((seq_count, columns), F32),
        ),
        in_specs=[pl.BlockSpec(memory_space=pltpu.SMEM)] + whole(5),
        out_specs=tuple(whole(2)),
    )(place, *parts, residual)


def combine_kernel(kept, mix, returned, out):
    picked = lax.dot_general(
        mix[...],
        returned[...].astype(F32),
        (((0,), (0,)), ((), ())),
        precision=lax.Precision.HIGHEST,
        preferred_element_type=F32,
    )
    out[...] = (kept[...] + picked).astype(BF16)


def combine(kept, mix, returned):
    return pl.pallas_call(
        combine_kernel,
        name="combine",
        out_shape=jax.ShapeDtypeStruct(kept.shape, BF16),
        in_specs=whole(3),
        out_specs=whole(1)[0],
    )(kept, mix, returned)


def passed_on(shard, step):
    devices = lax.axis_size("tp")
    return lax.ppermute(shard, "tp", [(i, (i + step) % devices) for i in range(devices)])


def shards(
    tokens,
    norm_gain,
    query_weight,
    key_weight,
    value_weight,
    output_weight,
    head_gain,
    lambdas,
    key_cache,
    value_cache,
    lengths,
    ffn_gain,
    routes,
    route_weight,
    expert_gate,
    expert_up,
    expert_down,
    dense_gate,
    dense_up,
    dense_down,
    gate_vector,
):
    seq_count, width = tokens.shape
    cache_len = key_cache.shape[1]
    devices = lax.axis_size("tp")
    experts_total = lax.axis_size("ep")
    slots = experts_total * CAP
    columns = width // devices
    place = lax.axis_index("tp").astype(jnp.int32).reshape(1)
    keys = jnp.transpose(key_cache, (0, 2, 1, 3)).reshape(seq_count, cache_len, 2 * DQK)
    values = jnp.transpose(value_cache, (0, 2, 1, 3)).reshape(seq_count, cache_len, DV)
    partial, dispatch, mix = attend(
        tokens, norm_gain[None], query_weight, key_weight, value_weight, output_weight,
        head_gain[None], lambdas, keys, values, lengths, routes.T, route_weight.T, slots,
    )
    parts = [partial] + [passed_on(partial, step) for step in range(1, devices)]
    residual, ffn_in, outbound = normalise(tokens, parts, ffn_gain[None], dispatch)
    arrived = lax.all_to_all(
        outbound.reshape(experts_total, CAP, width), "ep", split_axis=0, concat_axis=0, tiled=True
    )
    term, logit = dense_branch(ffn_in, dense_gate, dense_up, dense_down, gate_vector[None], columns)
    blocks = expert_rows(
        place, arrived.reshape(slots, width), expert_gate[0], expert_up[0], expert_down[0],
        term, logit, devices,
    )
    moved = [blocks[0]] + [passed_on(blocks[step], step) for step in range(1, devices)]
    summed, kept = gather_parts(place, moved, residual, slots)
    returned = lax.all_to_all(
        summed.reshape(experts_total, CAP, columns), "ep", split_axis=0, concat_axis=0, tiled=True
    )
    return combine(kept, mix, returned.reshape(slots, columns))


def solution(mesh):
    placed = (
        P("ep", None),
        P(),
        P(None, "tp"),
        P(None, "tp"),
        P(None, "tp"),
        P("tp", None),
        P(),
        P("tp"),
        P("ep", None, "tp", None),
        P("ep", None, "tp", None),
        P("ep"),
        P(),
        P("ep", None),
        P("ep", None),
        P("ep", None, "tp"),
        P("ep", None, "tp"),
        P("ep", "tp", None),
        P("tp", None),
        P("tp", None),
        P("tp", None),
        P("tp"),
    )
    return jax.shard_map(
        shards, mesh=mesh, in_specs=placed, out_specs=P("ep", "tp"), check_vma=False
    )
```

```python
import jax
import jax.numpy as jnp
from jax import lax
from jax.experimental import pallas as pl
from jax.experimental.pallas import tpu as pltpu
from jax.sharding import PartitionSpec as P

HEADS = 8
KV_HEADS = 4
DQK = 64
DV = 128
TOPK = 4
CAP = 2
GROUP = 4

epsilon = 1e-06
F32 = jnp.float32
BF16 = jnp.bfloat16


def rms_scale(values, gain):
    return values * lax.rsqrt(jnp.mean(values * values, axis=-1, keepdims=True) + epsilon) * gain


def dot(lhs, rhs, contract=((1,), (0,))):
    return lax.dot_general(lhs, rhs, (contract, ((), ())), preferred_element_type=F32)


def attention_kernel(
    lengths_hbm,
    lambdas_hbm,
    tokens_hbm,
    norm_gain_hbm,
    head_gain_hbm,
    query_hbm,
    key_hbm,
    value_hbm,
    output_hbm,
    key_cache,
    value_cache,
    partial_out,
    lengths,
    lambdas,
    tokens,
    norm_gain,
    head_gain,
    query_weight,
    key_weight,
    value_weight,
    output_weight,
    keys,
    values,
    mixture,
    sems,
):
    seq_count = tokens.shape[0]
    groups = seq_count // GROUP
    pairs = [
        (tokens_hbm, tokens),
        (norm_gain_hbm, norm_gain),
        (query_hbm, query_weight),
        (key_hbm, key_weight),
        (value_hbm, value_weight),
        (lengths_hbm, lengths),
        (lambdas_hbm, lambdas),
        (head_gain_hbm, head_gain),
    ]
    for group in range(groups):
        rows = pl.ds(group * GROUP, GROUP)
        pairs.append((key_cache.at[rows], keys.at[rows]))
        pairs.append((value_cache.at[rows], values.at[rows]))
    pairs.append((output_hbm, output_weight))
    copies = [
        pltpu.make_async_copy(source, target, sems.at[i])
        for i, (source, target) in enumerate(pairs)
    ]
    for copy in copies:
        copy.start()
    last = copies.pop()
    copies[0].wait()
    copies[1].wait()
    normed = rms_scale(tokens[...].astype(F32), norm_gain[...]).astype(BF16)
    copies[2].wait()
    queries = dot(normed, query_weight[...]).astype(BF16).astype(F32)
    copies[3].wait()
    new_keys = dot(normed, key_weight[...]).astype(BF16).astype(F32)
    copies[4].wait()
    new_values = dot(normed, value_weight[...]).astype(BF16).astype(F32)

    for copy in copies[5:8]:
        copy.wait()
    cache_len = keys.shape[1]
    row = lax.broadcasted_iota(jnp.int32, (8, 2 * DQK), 0)
    lane = lax.broadcasted_iota(jnp.int32, (8, 2 * DQK), 1)
    keep = jnp.logical_and((lane // DQK) == (row % 2), row < 4)
    row1 = lax.broadcasted_iota(jnp.int32, (8, 1), 0)
    sign = jnp.where(row1 % 2 == 0, 1.0, -jnp.where(row1 < 2, lambdas[0], lambdas[1]))
    position = lax.broadcasted_iota(jnp.int32, (8, cache_len), 1)
    score_scale = DQK ** (-0.5)
    for group in range(groups):
        copies[8 + 2 * group].wait()
        scores = []
        own_scores = []
        for s in range(group * GROUP, (group + 1) * GROUP):
            first = jnp.broadcast_to(queries[s : s + 1, : 2 * DQK], (8, 2 * DQK))
            second = jnp.broadcast_to(queries[s : s + 1, 2 * DQK :], (8, 2 * DQK))
            query = jnp.where(keep, jnp.where(row < 2, first, second), 0.0)
            score = dot(query.astype(BF16), keys[s], ((1,), (1,))) * score_scale
            scores.append(jnp.where(position < lengths[s], score, -jnp.inf))
            own_scores.append(
                jnp.sum(query * new_keys[s : s + 1, :], axis=1, keepdims=True) * score_scale
            )
        weights = []
        own_weights = []
        for score, own in zip(scores, own_scores):
            top = jnp.maximum(jnp.max(score, axis=1, keepdims=True), own)
            grown = jnp.exp(score - top)
            own_grown = jnp.exp(own - top)
            total = jnp.sum(grown, axis=1, keepdims=True) + own_grown
            share = sign / total
            prob = grown * share
            own_prob = own_grown * share
            weights.append((prob + pltpu.roll(prob, 7, 0)).astype(BF16))
            own_weights.append((own_prob + pltpu.roll(own_prob, 7, 0)).astype(BF16).astype(F32))
        copies[9 + 2 * group].wait()
        for i in range(GROUP):
            s = group * GROUP + i
            mixed = dot(weights[i], values[s]) + own_weights[i] * new_values[s : s + 1, :]
            mixture[s : s + 1, :DV] = mixed[0:1, :]
            mixture[s : s + 1, DV:] = mixed[2:3, :]
    gain = head_gain[...]
    left = rms_scale(mixture[:, :DV], gain).astype(BF16)
    right = rms_scale(mixture[:, DV:], gain).astype(BF16)
    last.wait()
    result = dot(left, output_weight[:DV, :]) + dot(right, output_weight[DV:, :])
    partial_out[...] = result.astype(BF16)


def whole(count):
    return [pl.BlockSpec(memory_space=pltpu.VMEM)] * count


def near(value):
    return pltpu.with_memory_space_constraint(value, pltpu.VMEM)


def all_far(*values):
    return [pltpu.with_memory_space_constraint(value, pltpu.HBM) for value in values]


def all_near(*values):
    return [near(value) for value in values]


def attend(lengths, lambdas, tokens, norm_gain, head_gain, query_weight, key_weight, value_weight,
           output_weight, key_cache, value_cache):
    seq_count, width = tokens.shape
    vectors = (tokens, norm_gain, head_gain, query_weight, key_weight, value_weight, output_weight,
               key_cache, value_cache)
    return pl.pallas_call(
        attention_kernel,
        name="attend",
        compiler_params=pltpu.CompilerParams(vmem_limit_bytes=16 << 20),
        out_shape=pltpu.VMEM((seq_count, width), BF16),
        in_specs=[pl.BlockSpec(memory_space=pltpu.HBM)] * 11,
        out_specs=whole(1)[0],
        scratch_shapes=[
            pltpu.SMEM(lengths.shape, lengths.dtype),
            pltpu.SMEM(lambdas.shape, lambdas.dtype),
            *[pltpu.VMEM(value.shape, value.dtype) for value in vectors],
            pltpu.VMEM((seq_count, 2 * DV), F32),
            pltpu.SemaphoreType.DMA((9 + 2 * (seq_count // GROUP),)),
        ],
    )(*all_far(lengths, lambdas, *vectors))


def load_kernel(*refs):
    count = (len(refs) - 2) // 2
    sems = refs[-1]
    copies = [
        pltpu.make_async_copy(refs[1 + i], refs[1 + count + i], sems.at[i]) for i in range(count)
    ]
    for copy in copies:
        copy.start()
    for copy in copies:
        copy.wait()


def load(after, *values):
    size = sum(value.size * value.dtype.itemsize for value in values)
    return pl.pallas_call(
        load_kernel,
        name="load",
        compiler_params=pltpu.CompilerParams(vmem_limit_bytes=4 << 20),
        out_shape=tuple(pltpu.VMEM(value.shape, value.dtype) for value in values),
        in_specs=whole(1) + [pl.BlockSpec(memory_space=pltpu.HBM)] * len(values),
        out_specs=tuple(whole(len(values))),
        scratch_shapes=[pltpu.SemaphoreType.DMA((len(values),))],
        cost_estimate=pl.CostEstimate(
            flops=1 << 30, bytes_accessed=size, transcendentals=0
        ),
    )(near(after), *all_far(*values))


def slot_masks(routes, route_weight, slots):
    seq_count = routes.shape[1]
    slot_ids = lax.broadcasted_iota(jnp.int32, (slots, seq_count), 0)
    named = jnp.zeros((slots, seq_count), F32)
    weighed = jnp.zeros((slots, seq_count), F32)
    for k in range(TOPK):
        hit = (slot_ids // CAP) == routes[k : k + 1, :]
        named = named + jnp.where(hit, 1.0, 0.0)
        weighed = weighed + jnp.where(hit, route_weight[k : k + 1, :], 0.0)
    before = lax.broadcasted_iota(jnp.int32, (seq_count, seq_count), 0)
    after = lax.broadcasted_iota(jnp.int32, (seq_count, seq_count), 1)
    earlier = jnp.where(before < after, 1.0, 0.0).astype(BF16)
    rank = dot(named.astype(BF16), earlier)
    chosen = rank == (slot_ids % CAP).astype(F32)
    return jnp.where(chosen, named, 0.0), jnp.where(chosen, weighed, 0.0)


def plan_kernel(routes, route_weight, dispatch, mix):
    named, weighed = slot_masks(routes, route_weight, dispatch.shape[0])
    dispatch[...] = named.astype(BF16)
    mix[...] = weighed


def plan(routes, route_weight, slots):
    seq_count = routes.shape[1]
    return pl.pallas_call(
        plan_kernel,
        name="plan",
        compiler_params=pltpu.CompilerParams(vmem_limit_bytes=4 << 20),
        out_shape=(pltpu.VMEM((slots, seq_count), BF16), pltpu.VMEM((slots, seq_count), F32)),
        in_specs=whole(2),
        out_specs=tuple(whole(2)),
        cost_estimate=pl.CostEstimate(flops=1 << 28, bytes_accessed=1 << 10, transcendentals=0),
    )(*all_near(routes, route_weight))


def normalise_kernel(
    tokens, own, one, two, three, gain, dispatch, residual, ffn_in, outbound
):
    attention = (own[...].astype(F32) + one[...].astype(F32)) + (
        two[...].astype(F32) + three[...].astype(F32)
    )
    total = tokens[...].astype(F32) + attention
    residual[...] = total
    ffn_in[...] = rms_scale(total, gain[...]).astype(BF16)
    columns = outbound.shape[2]
    start = pl.multiple_of(lax.axis_index("tp") * columns, columns)
    sent = dot(dispatch[...], ffn_in[:, pl.ds(start, columns)]).astype(BF16)
    outbound[...] = sent.reshape(outbound.shape)


def normalise(tokens, parts, gain, dispatch, columns):
    seq_count, width = tokens.shape
    return pl.pallas_call(
        normalise_kernel,
        name="normalise",
        compiler_params=pltpu.CompilerParams(vmem_limit_bytes=8 << 20),
        out_shape=(
            pltpu.VMEM((seq_count, width), F32),
            pltpu.VMEM((seq_count, width), BF16),
            pltpu.VMEM((dispatch.shape[0] // CAP, CAP, columns), BF16),
        ),
        in_specs=whole(7),
        out_specs=tuple(whole(3)),
    )(*all_near(tokens, *parts, gain, dispatch))


def silu(values):
    return values / (1.0 + jnp.exp(-values))


def dense_kernel(rows, gate, up, down, vector, term, logit):
    value = rows[...]
    gate_pre = dot(value, gate[...], ((1,), (1,)))
    up_proj = dot(value, up[...], ((1,), (1,)))
    hidden = (silu(gate_pre) * up_proj).astype(BF16)
    term[...] = dot(hidden, down[...]).astype(BF16)
    part = jnp.sum(hidden.astype(F32) * vector[...], axis=1, keepdims=True)
    high = part.astype(BF16)
    rest = part - high.astype(F32)
    middle = rest.astype(BF16)
    low = (rest - middle.astype(F32)).astype(BF16)
    lane = lax.broadcasted_iota(jnp.int32, logit.shape, 1)
    pieces = jnp.where(
        lane == 0, high.astype(F32), jnp.where(lane == 1, middle.astype(F32), low.astype(F32))
    )
    logit[...] = jnp.where(lane < 3, pieces, 0.0).astype(BF16)


def dense_branch(rows, gate, up, down, vector, columns):
    seq_count, width = rows.shape
    return pl.pallas_call(
        dense_kernel,
        name="dense",
        compiler_params=pltpu.CompilerParams(vmem_limit_bytes=8 << 20),
        out_shape=(
            pltpu.VMEM((seq_count, width), BF16),
            pltpu.VMEM((seq_count, columns), BF16),
        ),
        in_specs=whole(5),
        out_specs=tuple(whole(2)),
        cost_estimate=pl.CostEstimate(
            flops=6 * seq_count * width * gate.shape[0],
            bytes_accessed=6 * width * gate.shape[0],
            transcendentals=0,
        ),
    )(*all_near(rows, gate, up, down, vector))


def expert_kernel(own, one, two, three, gate, up, down, term, logit, *blocks):
    devices = len(blocks)
    place = lax.axis_index("tp")
    count, columns = own.shape[0] * own.shape[1], own.shape[2]
    seq_count = term.shape[0]
    gate_pre = jnp.zeros((count, gate.shape[1]), F32)
    up_proj = jnp.zeros((count, up.shape[1]), F32)
    for step, part in enumerate((own, one, two, three)):
        start = pl.multiple_of(((place + devices - step) % devices) * columns, columns)
        rows = part[...].reshape(count, columns)
        gate_pre = gate_pre + dot(rows, gate[pl.ds(start, columns), :])
        up_proj = up_proj + dot(rows, up[pl.ds(start, columns), :])
    hidden = (silu(gate_pre) * up_proj).astype(BF16)
    for step, block in enumerate(blocks):
        start = pl.multiple_of(((place + step) % devices) * columns, columns)
        block[:count, :] = dot(hidden, down[:, pl.ds(start, columns)]).astype(BF16)
        block[count : count + seq_count, :] = term[:, pl.ds(start, columns)]
        block[count + seq_count :, :] = logit[...]


def expert_rows(parts, gate, up, down, term, logit):
    devices = len(parts)
    experts, cap, columns = parts[0].shape
    shape = pltpu.VMEM((experts * cap + 2 * term.shape[0], columns), BF16)
    return pl.pallas_call(
        expert_kernel,
        name="experts",
        compiler_params=pltpu.CompilerParams(vmem_limit_bytes=8 << 20),
        out_shape=(shape,) * devices,
        in_specs=whole(9),
        out_specs=tuple(whole(devices)),
    )(*all_near(*parts, gate, up, down, term, logit))


def gather_kernel(own, one, two, three, residual, summed, kept):
    count, columns = summed.shape[0] * summed.shape[1], summed.shape[2]
    seq_count = residual.shape[0]
    total = (own[...].astype(F32) + one[...].astype(F32)) + (
        two[...].astype(F32) + three[...].astype(F32)
    )
    summed[...] = total[:count, :].astype(BF16).reshape(summed.shape)
    pieces = total[count + seq_count :, :]
    lane = lax.broadcasted_iota(jnp.int32, pieces.shape, 1)
    logit = jnp.sum(jnp.where(lane < 3, pieces, 0.0), axis=1, keepdims=True)
    gated = total[count : count + seq_count, :] / (1.0 + jnp.exp(-logit))
    start = pl.multiple_of(lax.axis_index("tp") * columns, columns)
    kept[...] = residual[:, pl.ds(start, columns)] + gated


def gather_parts(parts, residual, count):
    seq_count = residual.shape[0]
    columns = parts[0].shape[1]
    return pl.pallas_call(
        gather_kernel,
        name="gather",
        compiler_params=pltpu.CompilerParams(vmem_limit_bytes=8 << 20),
        out_shape=(
            pltpu.VMEM((count // CAP, CAP, columns), BF16),
            pltpu.VMEM((seq_count, columns), F32),
        ),
        in_specs=whole(5),
        out_specs=tuple(whole(2)),
    )(*all_near(*parts, residual))


def combine_kernel(kept, mix, returned, out):
    picked = lax.dot_general(
        mix[...],
        returned[...].reshape(mix.shape[0], -1).astype(F32),
        (((0,), (0,)), ((), ())),
        precision=lax.Precision.HIGHEST,
        preferred_element_type=F32,
    )
    out[...] = (kept[...] + picked).astype(BF16)


def combine(kept, mix, returned):
    return pl.pallas_call(
        combine_kernel,
        name="combine",
        compiler_params=pltpu.CompilerParams(vmem_limit_bytes=8 << 20),
        out_shape=jax.ShapeDtypeStruct(kept.shape, BF16),
        in_specs=whole(3),
        out_specs=whole(1)[0],
    )(*all_near(kept, mix, returned))


def passed_on(shard, step):
    devices = lax.axis_size("tp")
    return lax.ppermute(shard, "tp", [(i, (i + step) % devices) for i in range(devices)])


def shards(
    tokens,
    norm_gain,
    query_weight,
    key_weight,
    value_weight,
    output_weight,
    head_gain,
    lambdas,
    key_cache,
    value_cache,
    lengths,
    ffn_gain,
    routes,
    route_weight,
    expert_gate,
    expert_up,
    expert_down,
    dense_gate,
    dense_up,
    dense_down,
    gate_vector,
):
    seq_count, width = tokens.shape
    cache_len = key_cache.shape[1]
    devices = lax.axis_size("tp")
    experts_total = lax.axis_size("ep")
    slots = experts_total * CAP
    columns = width // devices
    keys = jnp.transpose(key_cache, (0, 2, 1, 3)).reshape(seq_count, cache_len, 2 * DQK)
    values = jnp.transpose(value_cache, (0, 2, 1, 3)).reshape(seq_count, cache_len, DV)
    partial = attend(
        lengths, lambdas, tokens, norm_gain[None], head_gain[None], query_weight, key_weight,
        value_weight, output_weight, keys, values,
    )
    parts = [partial] + [passed_on(partial, step) for step in range(1, devices)]
    (
        route_rows, weight_rows, near_tokens, near_gain, near_gate_vector,
        near_dense_gate, near_dense_up, near_dense_down,
        near_expert_gate, near_expert_up, near_expert_down,
    ) = load(
        partial, routes.T, route_weight.T, tokens, ffn_gain[None], gate_vector[None],
        dense_gate, dense_up, dense_down, expert_gate[0], expert_up[0], expert_down[0],
    )
    dispatch, mix = plan(route_rows, weight_rows, slots)
    residual, ffn_in, outbound = normalise(
        near_tokens, parts, near_gain, dispatch, columns
    )
    arrived = lax.all_to_all(outbound, "ep", split_axis=0, concat_axis=0, tiled=True)
    arrived, ffn_in = lax.optimization_barrier((arrived, ffn_in))
    term, logit = dense_branch(
        ffn_in, near_dense_gate, near_dense_up, near_dense_down, near_gate_vector, columns
    )
    gathered = [arrived] + [passed_on(arrived, step) for step in range(1, devices)]
    blocks = expert_rows(
        gathered, near_expert_gate, near_expert_up, near_expert_down, term, logit
    )
    moved = [blocks[0]] + [passed_on(blocks[step], step) for step in range(1, devices)]
    summed, kept = gather_parts(moved, residual, slots)
    returned = lax.all_to_all(summed, "ep", split_axis=0, concat_axis=0, tiled=True)
    return combine(kept, mix, returned)


def solution(mesh):
    placed = (
        P("ep", None),
        P(),
        P(None, "tp"),
        P(None, "tp"),
        P(None, "tp"),
        P("tp", None),
        P(),
        P("tp"),
        P("ep", None, "tp", None),
        P("ep", None, "tp", None),
        P("ep"),
        P(),
        P("ep", None),
        P("ep", None),
        P("ep", None, "tp"),
        P("ep", None, "tp"),
        P("ep", "tp", None),
        P("tp", None),
        P("tp", None),
        P("tp", None),
        P("tp"),
    )
    return jax.shard_map(
        shards, mesh=mesh, in_specs=placed, out_specs=P("ep", "tp"), check_vma=False
    )
```

```python
import jax
import jax.numpy as jnp
from jax import lax
from jax.experimental import pallas as pl
from jax.experimental.pallas import tpu as pltpu
from jax.sharding import PartitionSpec as P


DQK = 64
DV = 128
TOPK = 4
CAP = 2
GROUP = 4

epsilon = 1e-06
F32 = jnp.float32
BF16 = jnp.bfloat16


def rms_scale(values, gain):
    return values * lax.rsqrt(jnp.mean(values * values, axis=-1, keepdims=True) + epsilon) * gain


def dot(lhs, rhs, contract=((1,), (0,))):
    return lax.dot_general(lhs, rhs, (contract, ((), ())), preferred_element_type=F32)


def attention_kernel(
    lengths_hbm,
    lambdas_hbm,
    tokens_hbm,
    norm_gain_hbm,
    head_gain_hbm,
    query_hbm,
    key_hbm,
    value_hbm,
    output_hbm,
    key_cache,
    value_cache,
    partial_out,
    lengths,
    lambdas,
    tokens,
    norm_gain,
    head_gain,
    query_weight,
    key_weight,
    value_weight,
    output_weight,
    keys,
    values,
    mixture,
    sems,
):
    seq_count = tokens.shape[0]
    groups = seq_count // GROUP
    pairs = [
        (tokens_hbm, tokens),
        (norm_gain_hbm, norm_gain),
        (query_hbm, query_weight),
        (key_hbm, key_weight),
        (value_hbm, value_weight),
        (lengths_hbm, lengths),
        (lambdas_hbm, lambdas),
        (head_gain_hbm, head_gain),
    ]
    for group in range(groups):
        rows = pl.ds(group * GROUP, GROUP)
        pairs.append((key_cache.at[rows], keys.at[rows]))
        pairs.append((value_cache.at[rows], values.at[rows]))
    pairs.append((output_hbm, output_weight))
    copies = [
        pltpu.make_async_copy(source, target, sems.at[i])
        for i, (source, target) in enumerate(pairs)
    ]
    for copy in copies:
        copy.start()
    last = copies.pop()
    copies[0].wait()
    copies[1].wait()
    normed = rms_scale(tokens[...].astype(F32), norm_gain[...]).astype(BF16)
    copies[2].wait()
    queries = dot(normed, query_weight[...]).astype(BF16).astype(F32)
    copies[3].wait()
    new_keys = dot(normed, key_weight[...]).astype(BF16).astype(F32)
    copies[4].wait()
    new_values = dot(normed, value_weight[...]).astype(BF16).astype(F32)

    for copy in copies[5:8]:
        copy.wait()
    cache_len = keys.shape[1]
    row = lax.broadcasted_iota(jnp.int32, (8, 2 * DQK), 0)
    lane = lax.broadcasted_iota(jnp.int32, (8, 2 * DQK), 1)
    keep = jnp.logical_and((lane // DQK) == (row % 2), row < 4)
    row1 = lax.broadcasted_iota(jnp.int32, (8, 1), 0)
    sign = jnp.where(row1 % 2 == 0, 1.0, -jnp.where(row1 < 2, lambdas[0], lambdas[1]))
    position = lax.broadcasted_iota(jnp.int32, (8, cache_len), 1)
    score_scale = DQK ** (-0.5)
    for group in range(groups):
        copies[8 + 2 * group].wait()
        scores = []
        own_scores = []
        for s in range(group * GROUP, (group + 1) * GROUP):
            first = jnp.broadcast_to(queries[s : s + 1, : 2 * DQK], (8, 2 * DQK))
            second = jnp.broadcast_to(queries[s : s + 1, 2 * DQK :], (8, 2 * DQK))
            query = jnp.where(keep, jnp.where(row < 2, first, second), 0.0)
            score = dot(query.astype(BF16), keys[s], ((1,), (1,))) * score_scale
            scores.append(jnp.where(position < lengths[s], score, -jnp.inf))
            own_scores.append(
                jnp.sum(query * new_keys[s : s + 1, :], axis=1, keepdims=True) * score_scale
            )
        weights = []
        own_weights = []
        for score, own in zip(scores, own_scores):
            top = jnp.maximum(jnp.max(score, axis=1, keepdims=True), own)
            grown = jnp.exp(score - top)
            own_grown = jnp.exp(own - top)
            total = jnp.sum(grown, axis=1, keepdims=True) + own_grown
            share = sign / total
            prob = grown * share
            own_prob = own_grown * share
            weights.append((prob + pltpu.roll(prob, 7, 0)).astype(BF16))
            own_weights.append((own_prob + pltpu.roll(own_prob, 7, 0)).astype(BF16).astype(F32))
        copies[9 + 2 * group].wait()
        for i in range(GROUP):
            s = group * GROUP + i
            mixed = dot(weights[i], values[s]) + own_weights[i] * new_values[s : s + 1, :]
            mixture[s : s + 1, :DV] = mixed[0:1, :]
            mixture[s : s + 1, DV:] = mixed[2:3, :]
    gain = head_gain[...]
    left = rms_scale(mixture[:, :DV], gain).astype(BF16)
    right = rms_scale(mixture[:, DV:], gain).astype(BF16)
    last.wait()
    result = dot(left, output_weight[:DV, :]) + dot(right, output_weight[DV:, :])
    partial_out[...] = result.astype(BF16)


def whole(count):
    return [pl.BlockSpec(memory_space=pltpu.VMEM)] * count


def near(value):
    return pltpu.with_memory_space_constraint(value, pltpu.VMEM)


def all_far(*values):
    return [pltpu.with_memory_space_constraint(value, pltpu.HBM) for value in values]


def all_near(*values):
    return [near(value) for value in values]


def attend(lengths, lambdas, tokens, norm_gain, head_gain, query_weight, key_weight, value_weight,
           output_weight, key_cache, value_cache):
    seq_count, width = tokens.shape
    vectors = (tokens, norm_gain, head_gain, query_weight, key_weight, value_weight, output_weight,
               key_cache, value_cache)
    return pl.pallas_call(
        attention_kernel,
        name="attend",
        compiler_params=pltpu.CompilerParams(vmem_limit_bytes=16 << 20),
        out_shape=pltpu.VMEM((seq_count, width), BF16),
        in_specs=[pl.BlockSpec(memory_space=pltpu.HBM)] * 11,
        out_specs=whole(1)[0],
        scratch_shapes=[
            pltpu.SMEM(lengths.shape, lengths.dtype),
            pltpu.SMEM(lambdas.shape, lambdas.dtype),
            *[pltpu.VMEM(value.shape, value.dtype) for value in vectors],
            pltpu.VMEM((seq_count, 2 * DV), F32),
            pltpu.SemaphoreType.DMA((9 + 2 * (seq_count // GROUP),)),
        ],
    )(*all_far(lengths, lambdas, *vectors))


def load_kernel(*refs):
    count = (len(refs) - 2) // 2
    sems = refs[-1]
    copies = [
        pltpu.make_async_copy(refs[1 + i], refs[1 + count + i], sems.at[i]) for i in range(count)
    ]
    for copy in copies:
        copy.start()
    for copy in copies:
        copy.wait()


def load(after, *values):
    size = sum(value.size * value.dtype.itemsize for value in values)
    return pl.pallas_call(
        load_kernel,
        name="load",
        compiler_params=pltpu.CompilerParams(vmem_limit_bytes=4 << 20),
        out_shape=tuple(pltpu.VMEM(value.shape, value.dtype) for value in values),
        in_specs=whole(1) + [pl.BlockSpec(memory_space=pltpu.HBM)] * len(values),
        out_specs=tuple(whole(len(values))),
        scratch_shapes=[pltpu.SemaphoreType.DMA((len(values),))],
        cost_estimate=pl.CostEstimate(
            flops=1 << 30, bytes_accessed=size, transcendentals=0
        ),
    )(near(after), *all_far(*values))


def slot_masks(routes, route_weight, slots):
    seq_count = routes.shape[1]
    slot_ids = lax.broadcasted_iota(jnp.int32, (slots, seq_count), 0)
    named = jnp.zeros((slots, seq_count), F32)
    weighed = jnp.zeros((slots, seq_count), F32)
    for k in range(TOPK):
        hit = (slot_ids // CAP) == routes[k : k + 1, :]
        named = named + jnp.where(hit, 1.0, 0.0)
        weighed = weighed + jnp.where(hit, route_weight[k : k + 1, :], 0.0)
    before = lax.broadcasted_iota(jnp.int32, (seq_count, seq_count), 0)
    after = lax.broadcasted_iota(jnp.int32, (seq_count, seq_count), 1)
    earlier = jnp.where(before < after, 1.0, 0.0).astype(BF16)
    rank = dot(named.astype(BF16), earlier)
    chosen = rank == (slot_ids % CAP).astype(F32)
    return jnp.where(chosen, named, 0.0), jnp.where(chosen, weighed, 0.0)


def plan_kernel(routes, route_weight, dispatch, mix):
    named, weighed = slot_masks(routes, route_weight, dispatch.shape[0])
    dispatch[...] = named.astype(BF16)
    mix[...] = weighed


def plan(routes, route_weight, slots):
    seq_count = routes.shape[1]
    return pl.pallas_call(
        plan_kernel,
        name="plan",
        compiler_params=pltpu.CompilerParams(vmem_limit_bytes=4 << 20),
        out_shape=(pltpu.VMEM((slots, seq_count), BF16), pltpu.VMEM((slots, seq_count), F32)),
        in_specs=whole(2),
        out_specs=tuple(whole(2)),
        cost_estimate=pl.CostEstimate(flops=1 << 28, bytes_accessed=1 << 10, transcendentals=0),
    )(*all_near(routes, route_weight))


def normalise_kernel(
    tokens, own, one, two, three, gain, dispatch, residual, ffn_in, outbound
):
    attention = (own[...].astype(F32) + one[...].astype(F32)) + (
        two[...].astype(F32) + three[...].astype(F32)
    )
    total = tokens[...].astype(F32) + attention
    residual[...] = total
    ffn_in[...] = rms_scale(total, gain[...]).astype(BF16)
    columns = outbound.shape[2]
    start = pl.multiple_of(lax.axis_index("tp") * columns, columns)
    sent = dot(dispatch[...], ffn_in[:, pl.ds(start, columns)]).astype(BF16)
    outbound[...] = sent.reshape(outbound.shape)


def normalise(tokens, parts, gain, dispatch, columns):
    seq_count, width = tokens.shape
    return pl.pallas_call(
        normalise_kernel,
        name="normalise",
        compiler_params=pltpu.CompilerParams(vmem_limit_bytes=8 << 20),
        out_shape=(
            pltpu.VMEM((seq_count, width), F32),
            pltpu.VMEM((seq_count, width), BF16),
            pltpu.VMEM((dispatch.shape[0] // CAP, CAP, columns), BF16),
        ),
        in_specs=whole(7),
        out_specs=tuple(whole(3)),
    )(*all_near(tokens, *parts, gain, dispatch))


def silu(values):
    return values / (1.0 + jnp.exp(-values))


def dense_kernel(rows, gate, up, down, vector, *refs):
    far, near_refs, blocks, sems = refs[:3], refs[3:6], refs[6:-1], refs[-1]
    copies = [
        pltpu.make_async_copy(source, target, sems.at[i])
        for i, (source, target) in enumerate(zip(far, near_refs))
    ]
    for copy in copies:
        copy.start()
    devices = len(blocks)
    seq_count, columns = rows.shape[0], blocks[0].shape[1]
    place = lax.axis_index("tp")
    value = rows[...]
    gate_pre = dot(value, gate[...], ((1,), (1,)))
    up_proj = dot(value, up[...], ((1,), (1,)))
    hidden = (silu(gate_pre) * up_proj).astype(BF16)
    part = jnp.sum(hidden.astype(F32) * vector[...], axis=1, keepdims=True)
    high = part.astype(BF16)
    rest = part - high.astype(F32)
    middle = rest.astype(BF16)
    low = (rest - middle.astype(F32)).astype(BF16)
    lane = lax.broadcasted_iota(jnp.int32, (seq_count, columns), 1)
    pieces = jnp.where(
        lane == 0, high.astype(F32), jnp.where(lane == 1, middle.astype(F32), low.astype(F32))
    )
    logit = jnp.where(lane < 3, pieces, 0.0).astype(BF16)
    for step, block in enumerate(blocks):
        start = pl.multiple_of(((place + step) % devices) * columns, columns)
        block[:seq_count, :] = dot(hidden, down[:, pl.ds(start, columns)]).astype(BF16)
        block[seq_count:, :] = logit
    for copy in copies:
        copy.wait()


def dense_branch(rows, gate, up, down, vector, expert_weights, devices):
    seq_count, width = rows.shape
    block = pltpu.VMEM((2 * seq_count, width // devices), BF16)
    outs = pl.pallas_call(
        dense_kernel,
        name="dense",
        compiler_params=pltpu.CompilerParams(vmem_limit_bytes=8 << 20),
        out_shape=tuple(pltpu.VMEM(value.shape, value.dtype) for value in expert_weights)
        + (block,) * devices,
        in_specs=whole(5) + [pl.BlockSpec(memory_space=pltpu.HBM)] * 3,
        out_specs=tuple(whole(3 + devices)),
        scratch_shapes=[pltpu.SemaphoreType.DMA((3,))],
        cost_estimate=pl.CostEstimate(
            flops=6 * seq_count * width * gate.shape[0],
            bytes_accessed=6 * width * gate.shape[0],
            transcendentals=0,
        ),
    )(*all_near(rows, gate, up, down, vector), *all_far(*expert_weights))
    return outs[:3], outs[3:]


def expert_kernel(own, one, two, three, gate, up, down, *blocks):
    devices = len(blocks)
    place = lax.axis_index("tp")
    count, columns = own.shape[0] * own.shape[1], own.shape[2]
    gate_pre = jnp.zeros((count, gate.shape[1]), F32)
    up_proj = jnp.zeros((count, up.shape[1]), F32)
    for step, part in enumerate((own, one, two, three)):
        start = pl.multiple_of(((place + devices - step) % devices) * columns, columns)
        rows = part[...].reshape(count, columns)
        gate_pre = gate_pre + dot(rows, gate[pl.ds(start, columns), :])
        up_proj = up_proj + dot(rows, up[pl.ds(start, columns), :])
    hidden = (silu(gate_pre) * up_proj).astype(BF16)
    for step, block in enumerate(blocks):
        start = pl.multiple_of(((place + step) % devices) * columns, columns)
        block[...] = dot(hidden, down[:, pl.ds(start, columns)]).astype(BF16)


def expert_rows(parts, gate, up, down):
    devices = len(parts)
    experts, cap, columns = parts[0].shape
    return pl.pallas_call(
        expert_kernel,
        name="experts",
        compiler_params=pltpu.CompilerParams(vmem_limit_bytes=8 << 20),
        out_shape=(pltpu.VMEM((experts * cap, columns), BF16),) * devices,
        in_specs=whole(7),
        out_specs=tuple(whole(devices)),
    )(*all_near(*parts, gate, up, down))


def gather_kernel(own, one, two, three, dense_own, dense_one, dense_two, dense_three, residual,
                  summed, kept):
    columns = summed.shape[2]
    seq_count = residual.shape[0]
    total = (own[...].astype(F32) + one[...].astype(F32)) + (
        two[...].astype(F32) + three[...].astype(F32)
    )
    summed[...] = total.astype(BF16).reshape(summed.shape)
    dense = (dense_own[...].astype(F32) + dense_one[...].astype(F32)) + (
        dense_two[...].astype(F32) + dense_three[...].astype(F32)
    )
    pieces = dense[seq_count:, :]
    lane = lax.broadcasted_iota(jnp.int32, pieces.shape, 1)
    logit = jnp.sum(jnp.where(lane < 3, pieces, 0.0), axis=1, keepdims=True)
    gated = dense[:seq_count, :] / (1.0 + jnp.exp(-logit))
    start = pl.multiple_of(lax.axis_index("tp") * columns, columns)
    kept[...] = residual[:, pl.ds(start, columns)] + gated


def gather_parts(parts, dense_parts, residual, count):
    seq_count = residual.shape[0]
    columns = parts[0].shape[1]
    return pl.pallas_call(
        gather_kernel,
        name="gather",
        compiler_params=pltpu.CompilerParams(vmem_limit_bytes=8 << 20),
        out_shape=(
            pltpu.VMEM((count // CAP, CAP, columns), BF16),
            pltpu.VMEM((seq_count, columns), F32),
        ),
        in_specs=whole(9),
        out_specs=tuple(whole(2)),
    )(*all_near(*parts, *dense_parts, residual))


def combine_kernel(kept, mix, returned, out):
    picked = lax.dot_general(
        mix[...],
        returned[...].reshape(mix.shape[0], -1).astype(F32),
        (((0,), (0,)), ((), ())),
        precision=lax.Precision.HIGHEST,
        preferred_element_type=F32,
    )
    out[...] = (kept[...] + picked).astype(BF16)


def combine(kept, mix, returned):
    return pl.pallas_call(
        combine_kernel,
        name="combine",
        compiler_params=pltpu.CompilerParams(vmem_limit_bytes=8 << 20),
        out_shape=jax.ShapeDtypeStruct(kept.shape, BF16),
        in_specs=whole(3),
        out_specs=whole(1)[0],
    )(*all_near(kept, mix, returned))


def passed_on(shard, step):
    devices = lax.axis_size("tp")
    return lax.ppermute(shard, "tp", [(i, (i + step) % devices) for i in range(devices)])


def shards(
    tokens,
    norm_gain,
    query_weight,
    key_weight,
    value_weight,
    output_weight,
    head_gain,
    lambdas,
    key_cache,
    value_cache,
    lengths,
    ffn_gain,
    routes,
    route_weight,
    expert_gate,
    expert_up,
    expert_down,
    dense_gate,
    dense_up,
    dense_down,
    gate_vector,
):
    seq_count, width = tokens.shape
    cache_len = key_cache.shape[1]
    devices = lax.axis_size("tp")
    experts_total = lax.axis_size("ep")
    slots = experts_total * CAP
    columns = width // devices
    keys = jnp.transpose(key_cache, (0, 2, 1, 3)).reshape(seq_count, cache_len, 2 * DQK)
    values = jnp.transpose(value_cache, (0, 2, 1, 3)).reshape(seq_count, cache_len, DV)
    partial = attend(
        lengths, lambdas, tokens, norm_gain[None], head_gain[None], query_weight, key_weight,
        value_weight, output_weight, keys, values,
    )
    parts = [partial] + [passed_on(partial, step) for step in range(1, devices)]
    (
        route_rows, weight_rows, near_tokens, near_gain, near_gate_vector,
        near_dense_gate, near_dense_up, near_dense_down,
    ) = load(
        partial, routes.T, route_weight.T, tokens, ffn_gain[None], gate_vector[None],
        dense_gate, dense_up, dense_down,
    )
    dispatch, mix = plan(route_rows, weight_rows, slots)
    residual, ffn_in, outbound = normalise(
        near_tokens, parts, near_gain, dispatch, columns
    )
    arrived = lax.all_to_all(outbound, "ep", split_axis=0, concat_axis=0, tiled=True)
    arrived, ffn_in = lax.optimization_barrier((arrived, ffn_in))
    gathered = [arrived] + [passed_on(arrived, step) for step in range(1, devices)]
    expert_weights, dense_blocks = dense_branch(
        ffn_in, near_dense_gate, near_dense_up, near_dense_down, near_gate_vector,
        (expert_gate[0], expert_up[0], expert_down[0]), devices,
    )
    dense_moved = [dense_blocks[0]]
    for step in range(1, devices):
        dense_moved.append(passed_on(dense_blocks[step], step))
    blocks = expert_rows(gathered, *expert_weights)
    moved = [blocks[0]] + [passed_on(blocks[step], step) for step in range(1, devices)]
    summed, kept = gather_parts(moved, dense_moved, residual, slots)
    returned = lax.all_to_all(summed, "ep", split_axis=0, concat_axis=0, tiled=True)
    return combine(kept, mix, returned)


def solution(mesh):
    placed = (
        P("ep", None),
        P(),
        P(None, "tp"),
        P(None, "tp"),
        P(None, "tp"),
        P("tp", None),
        P(),
        P("tp"),
        P("ep", None, "tp", None),
        P("ep", None, "tp", None),
        P("ep"),
        P(),
        P("ep", None),
        P("ep", None),
        P("ep", None, "tp"),
        P("ep", None, "tp"),
        P("ep", "tp", None),
        P("tp", None),
        P("tp", None),
        P("tp", None),
        P("tp"),
    )

    return jax.shard_map(
        shards, mesh=mesh, in_specs=placed, out_specs=P("ep", "tp"), check_vma=False
    )
```

```python
import jax
import jax.numpy as jnp
from jax import lax
from jax.experimental import pallas as pl
from jax.experimental.pallas import tpu as pltpu
from jax.sharding import PartitionSpec as P


DQK = 64
DV = 128
TOPK = 4
CAP = 2
GROUP = 8

epsilon = 1e-06
F32 = jnp.float32
BF16 = jnp.bfloat16


def rms_scale(values, gain):
    return values * lax.rsqrt(jnp.mean(values * values, axis=-1, keepdims=True) + epsilon) * gain


def dot(lhs, rhs, contract=((1,), (0,))):
    return lax.dot_general(lhs, rhs, (contract, ((), ())), preferred_element_type=F32)


def attention_kernel(
    lengths_hbm,
    lambdas_hbm,
    tokens_hbm,
    norm_gain_hbm,
    head_gain_hbm,
    query_hbm,
    key_hbm,
    value_hbm,
    output_hbm,
    key_cache,
    value_cache,
    partial_out,
    lengths,
    lambdas,
    tokens,
    norm_gain,
    head_gain,
    query_weight,
    key_weight,
    value_weight,
    output_weight,
    keys,
    values,
    mixture,
    sems,
):
    seq_count = tokens.shape[0]
    groups = seq_count // GROUP
    pairs = [
        (tokens_hbm, tokens),
        (norm_gain_hbm, norm_gain),
        (query_hbm, query_weight),
        (key_hbm, key_weight),
        (value_hbm, value_weight),
        (lengths_hbm, lengths),
        (lambdas_hbm, lambdas),
        (head_gain_hbm, head_gain),
    ]
    for group in range(groups):
        rows = pl.ds(group * GROUP, GROUP)
        pairs.append((key_cache.at[rows], keys.at[rows]))
        pairs.append((value_cache.at[rows], values.at[rows]))
    pairs.append((output_hbm, output_weight))
    copies = [
        pltpu.make_async_copy(source, target, sems.at[i])
        for i, (source, target) in enumerate(pairs)
    ]
    for copy in copies:
        copy.start()
    last = copies.pop()
    copies[0].wait()
    copies[1].wait()
    normed = rms_scale(tokens[...].astype(F32), norm_gain[...]).astype(BF16)
    copies[2].wait()
    queries = dot(normed, query_weight[...]).astype(BF16).astype(F32)
    copies[3].wait()
    new_keys = dot(normed, key_weight[...]).astype(BF16).astype(F32)
    copies[4].wait()
    new_values = dot(normed, value_weight[...]).astype(BF16).astype(F32)

    for copy in copies[5:8]:
        copy.wait()
    cache_len = keys.shape[1]
    row = lax.broadcasted_iota(jnp.int32, (8, 2 * DQK), 0)
    lane = lax.broadcasted_iota(jnp.int32, (8, 2 * DQK), 1)
    keep = jnp.logical_and((lane // DQK) == (row % 2), row < 4)
    row1 = lax.broadcasted_iota(jnp.int32, (8, 1), 0)
    sign = jnp.where(row1 % 2 == 0, 1.0, -jnp.where(row1 < 2, lambdas[0], lambdas[1]))
    position = lax.broadcasted_iota(jnp.int32, (8, cache_len), 1)
    score_scale = DQK ** (-0.5)
    for group in range(groups):
        copies[8 + 2 * group].wait()
        scores = []
        own_scores = []
        for s in range(group * GROUP, (group + 1) * GROUP):
            first = jnp.broadcast_to(queries[s : s + 1, : 2 * DQK], (8, 2 * DQK))
            second = jnp.broadcast_to(queries[s : s + 1, 2 * DQK :], (8, 2 * DQK))
            query = jnp.where(keep, jnp.where(row < 2, first, second), 0.0)
            score = dot(query.astype(BF16), keys[s], ((1,), (1,))) * score_scale
            scores.append(jnp.where(position < lengths[s], score, -jnp.inf))
            own_scores.append(
                jnp.sum(query * new_keys[s : s + 1, :], axis=1, keepdims=True) * score_scale
            )
        weights = []
        own_weights = []
        for score, own in zip(scores, own_scores):
            top = jnp.maximum(jnp.max(score, axis=1, keepdims=True), own)
            grown = jnp.exp(score - top)
            own_grown = jnp.exp(own - top)
            total = jnp.sum(grown, axis=1, keepdims=True) + own_grown
            share = sign / total
            prob = grown * share
            own_prob = own_grown * share
            weights.append((prob + pltpu.roll(prob, 7, 0)).astype(BF16))
            own_weights.append((own_prob + pltpu.roll(own_prob, 7, 0)).astype(BF16).astype(F32))
        copies[9 + 2 * group].wait()
        for i in range(GROUP):
            s = group * GROUP + i
            mixed = dot(weights[i], values[s]) + own_weights[i] * new_values[s : s + 1, :]
            mixture[s : s + 1, :DV] = mixed[0:1, :]
            mixture[s : s + 1, DV:] = mixed[2:3, :]
    gain = head_gain[...]
    left = rms_scale(mixture[:, :DV], gain).astype(BF16)
    right = rms_scale(mixture[:, DV:], gain).astype(BF16)
    last.wait()
    result = dot(left, output_weight[:DV, :]) + dot(right, output_weight[DV:, :])
    partial_out[...] = result.astype(BF16)


def whole(count):
    return [pl.BlockSpec(memory_space=pltpu.VMEM)] * count


def near(value):
    return pltpu.with_memory_space_constraint(value, pltpu.VMEM)


def all_far(*values):
    return [pltpu.with_memory_space_constraint(value, pltpu.HBM) for value in values]


def all_near(*values):
    return [near(value) for value in values]


def attend(lengths, lambdas, tokens, norm_gain, head_gain, query_weight, key_weight, value_weight,
           output_weight, key_cache, value_cache):
    seq_count, width = tokens.shape
    vectors = (tokens, norm_gain, head_gain, query_weight, key_weight, value_weight, output_weight,
               key_cache, value_cache)
    return pl.pallas_call(
        attention_kernel,
        name="attend",
        compiler_params=pltpu.CompilerParams(vmem_limit_bytes=16 << 20),
        out_shape=pltpu.VMEM((seq_count, width), BF16),
        in_specs=[pl.BlockSpec(memory_space=pltpu.HBM)] * 11,
        out_specs=whole(1)[0],
        scratch_shapes=[
            pltpu.SMEM(lengths.shape, lengths.dtype),
            pltpu.SMEM(lambdas.shape, lambdas.dtype),
            *[pltpu.VMEM(value.shape, value.dtype) for value in vectors],
            pltpu.VMEM((seq_count, 2 * DV), F32),
            pltpu.SemaphoreType.DMA((9 + 2 * (seq_count // GROUP),)),
        ],
    )(*all_far(lengths, lambdas, *vectors))


def load_kernel(*refs):
    count = (len(refs) - 2) // 2
    sems = refs[-1]
    copies = [
        pltpu.make_async_copy(refs[1 + i], refs[1 + count + i], sems.at[i]) for i in range(count)
    ]
    for copy in copies:
        copy.start()
    for copy in copies:
        copy.wait()


def load(after, *values):
    size = sum(value.size * value.dtype.itemsize for value in values)
    return pl.pallas_call(
        load_kernel,
        name="load",
        compiler_params=pltpu.CompilerParams(vmem_limit_bytes=4 << 20),
        out_shape=tuple(pltpu.VMEM(value.shape, value.dtype) for value in values),
        in_specs=whole(1) + [pl.BlockSpec(memory_space=pltpu.HBM)] * len(values),
        out_specs=tuple(whole(len(values))),
        scratch_shapes=[pltpu.SemaphoreType.DMA((len(values),))],
        cost_estimate=pl.CostEstimate(
            flops=1 << 30, bytes_accessed=size, transcendentals=0
        ),
    )(near(after), *all_far(*values))


def slot_masks(routes, route_weight, slots):
    seq_count = routes.shape[1]
    slot_ids = lax.broadcasted_iota(jnp.int32, (slots, seq_count), 0)
    named = jnp.zeros((slots, seq_count), F32)
    weighed = jnp.zeros((slots, seq_count), F32)
    for k in range(TOPK):
        hit = (slot_ids // CAP) == routes[k : k + 1, :]
        named = named + jnp.where(hit, 1.0, 0.0)
        weighed = weighed + jnp.where(hit, route_weight[k : k + 1, :], 0.0)
    before = lax.broadcasted_iota(jnp.int32, (seq_count, seq_count), 0)
    after = lax.broadcasted_iota(jnp.int32, (seq_count, seq_count), 1)
    earlier = jnp.where(before < after, 1.0, 0.0).astype(BF16)
    rank = dot(named.astype(BF16), earlier)
    chosen = rank == (slot_ids % CAP).astype(F32)
    return jnp.where(chosen, named, 0.0), jnp.where(chosen, weighed, 0.0)


def three_pieces(values):
    high = values.astype(BF16)
    rest = values - high.astype(F32)
    middle = rest.astype(BF16)
    return high, middle, (rest - middle.astype(F32)).astype(BF16)


def plan_kernel(routes, route_weight, dispatch, mix):
    named, weighed = slot_masks(routes, route_weight, dispatch.shape[0])
    dispatch[...] = named.astype(BF16)
    for i, piece in enumerate(three_pieces(weighed.T)):
        mix[i] = piece


def plan(routes, route_weight, slots):
    seq_count = routes.shape[1]
    return pl.pallas_call(
        plan_kernel,
        name="plan",
        compiler_params=pltpu.CompilerParams(vmem_limit_bytes=4 << 20),
        out_shape=(pltpu.VMEM((slots, seq_count), BF16), pltpu.VMEM((3, seq_count, slots), BF16)),
        in_specs=whole(2),
        out_specs=tuple(whole(2)),
        cost_estimate=pl.CostEstimate(flops=1 << 28, bytes_accessed=1 << 10, transcendentals=0),
    )(*all_near(routes, route_weight))


def normalise_kernel(
    tokens, own, one, two, three, gain, dispatch, residual, ffn_in, outbound
):
    attention = (own[...].astype(F32) + one[...].astype(F32)) + (
        two[...].astype(F32) + three[...].astype(F32)
    )
    total = tokens[...].astype(F32) + attention
    residual[...] = total
    ffn_in[...] = rms_scale(total, gain[...]).astype(BF16)
    columns = outbound.shape[2]
    start = pl.multiple_of(lax.axis_index("tp") * columns, columns)
    sent = dot(dispatch[...], ffn_in[:, pl.ds(start, columns)]).astype(BF16)
    outbound[...] = sent.reshape(outbound.shape)


def normalise(tokens, parts, gain, dispatch, columns):
    seq_count, width = tokens.shape
    return pl.pallas_call(
        normalise_kernel,
        name="normalise",
        compiler_params=pltpu.CompilerParams(vmem_limit_bytes=8 << 20),
        out_shape=(
            pltpu.VMEM((seq_count, width), F32),
            pltpu.VMEM((seq_count, width), BF16),
            pltpu.VMEM((dispatch.shape[0] // CAP, CAP, columns), BF16),
        ),
        in_specs=whole(7),
        out_specs=tuple(whole(3)),
    )(*all_near(tokens, *parts, gain, dispatch))


def silu(values):
    return values / (1.0 + jnp.exp(-values))


def dense_kernel(rows, gate, up, down, vector, *refs):
    far, near_refs, blocks, sems = refs[:3], refs[3:6], refs[6:-1], refs[-1]
    copies = [
        pltpu.make_async_copy(source, target, sems.at[i])
        for i, (source, target) in enumerate(zip(far, near_refs))
    ]
    for copy in copies:
        copy.start()
    devices = len(blocks)
    seq_count, columns = rows.shape[0], blocks[0].shape[1]
    place = lax.axis_index("tp")
    value = rows[...]
    gate_pre = dot(value, gate[...], ((1,), (1,)))
    up_proj = dot(value, up[...], ((1,), (1,)))
    hidden = (silu(gate_pre) * up_proj).astype(BF16)
    part = jnp.sum(hidden.astype(F32) * vector[...], axis=1, keepdims=True)
    high, middle, low = three_pieces(part)
    lane = lax.broadcasted_iota(jnp.int32, (seq_count, columns), 1)
    pieces = jnp.where(
        lane == 0, high.astype(F32), jnp.where(lane == 1, middle.astype(F32), low.astype(F32))
    )
    logit = jnp.where(lane < 3, pieces, 0.0).astype(BF16)
    for step, block in enumerate(blocks):
        start = pl.multiple_of(((place + step) % devices) * columns, columns)
        block[:seq_count, :] = dot(hidden, down[:, pl.ds(start, columns)]).astype(BF16)
        block[seq_count:, :] = logit
    for copy in copies:
        copy.wait()


def dense_branch(rows, gate, up, down, vector, expert_weights, devices):
    seq_count, width = rows.shape
    block = pltpu.VMEM((2 * seq_count, width // devices), BF16)
    outs = pl.pallas_call(
        dense_kernel,
        name="dense",
        compiler_params=pltpu.CompilerParams(vmem_limit_bytes=8 << 20),
        out_shape=tuple(pltpu.VMEM(value.shape, value.dtype) for value in expert_weights)
        + (block,) * devices,
        in_specs=whole(5) + [pl.BlockSpec(memory_space=pltpu.HBM)] * 3,
        out_specs=tuple(whole(3 + devices)),
        scratch_shapes=[pltpu.SemaphoreType.DMA((3,))],
        cost_estimate=pl.CostEstimate(
            flops=6 * seq_count * width * gate.shape[0],
            bytes_accessed=6 * width * gate.shape[0],
            transcendentals=0,
        ),
    )(*all_near(rows, gate, up, down, vector), *all_far(*expert_weights))
    return outs[:3], outs[3:]


def expert_kernel(own, one, two, three, gate, up, down, *blocks):
    devices = len(blocks)
    place = lax.axis_index("tp")
    count, columns = own.shape[0] * own.shape[1], own.shape[2]
    gate_pre = jnp.zeros((count, gate.shape[1]), F32)
    up_proj = jnp.zeros((count, up.shape[1]), F32)
    for step, part in enumerate((own, one, two, three)):
        start = pl.multiple_of(((place + devices - step) % devices) * columns, columns)
        rows = part[...].reshape(count, columns)
        gate_pre = gate_pre + dot(rows, gate[pl.ds(start, columns), :])
        up_proj = up_proj + dot(rows, up[pl.ds(start, columns), :])
    hidden = (silu(gate_pre) * up_proj).astype(BF16)
    for step, block in enumerate(blocks):
        start = pl.multiple_of(((place + step) % devices) * columns, columns)
        block[...] = dot(hidden, down[:, pl.ds(start, columns)]).astype(BF16)


def expert_rows(parts, gate, up, down):
    devices = len(parts)
    experts, cap, columns = parts[0].shape
    return pl.pallas_call(
        expert_kernel,
        name="experts",
        compiler_params=pltpu.CompilerParams(vmem_limit_bytes=8 << 20),
        out_shape=(pltpu.VMEM((experts * cap, columns), BF16),) * devices,
        in_specs=whole(7),
        out_specs=tuple(whole(devices)),
    )(*all_near(*parts, gate, up, down))


def gather_kernel(own, one, two, three, dense_own, dense_one, dense_two, dense_three, residual,
                  summed, kept):
    columns = summed.shape[2]
    seq_count = residual.shape[0]
    total = (own[...].astype(F32) + one[...].astype(F32)) + (
        two[...].astype(F32) + three[...].astype(F32)
    )
    summed[...] = total.astype(BF16).reshape(summed.shape)
    dense = (dense_own[...].astype(F32) + dense_one[...].astype(F32)) + (
        dense_two[...].astype(F32) + dense_three[...].astype(F32)
    )
    pieces = dense[seq_count:, :]
    lane = lax.broadcasted_iota(jnp.int32, pieces.shape, 1)
    logit = jnp.sum(jnp.where(lane < 3, pieces, 0.0), axis=1, keepdims=True)
    gated = dense[:seq_count, :] / (1.0 + jnp.exp(-logit))
    start = pl.multiple_of(lax.axis_index("tp") * columns, columns)
    kept[...] = residual[:, pl.ds(start, columns)] + gated


def gather_parts(parts, dense_parts, residual, count):
    seq_count = residual.shape[0]
    columns = parts[0].shape[1]
    return pl.pallas_call(
        gather_kernel,
        name="gather",
        compiler_params=pltpu.CompilerParams(vmem_limit_bytes=8 << 20),
        out_shape=(
            pltpu.VMEM((count // CAP, CAP, columns), BF16),
            pltpu.VMEM((seq_count, columns), F32),
        ),
        in_specs=whole(9),
        out_specs=tuple(whole(2)),
    )(*all_near(*parts, *dense_parts, residual))


def combine_kernel(kept, mix, returned, out):
    rows = returned[...].reshape(mix.shape[2], -1)
    picked = dot(mix[0], rows) + (dot(mix[1], rows) + dot(mix[2], rows))
    out[...] = (kept[...] + picked).astype(BF16)


def combine(kept, mix, returned):
    return pl.pallas_call(
        combine_kernel,
        name="combine",
        compiler_params=pltpu.CompilerParams(vmem_limit_bytes=8 << 20),
        out_shape=jax.ShapeDtypeStruct(kept.shape, BF16),
        in_specs=whole(3),
        out_specs=whole(1)[0],
    )(*all_near(kept, mix, returned))


def passed_on(shard, step):
    devices = lax.axis_size("tp")
    return lax.ppermute(shard, "tp", [(i, (i + step) % devices) for i in range(devices)])


def shards(
    tokens,
    norm_gain,
    query_weight,
    key_weight,
    value_weight,
    output_weight,
    head_gain,
    lambdas,
    key_cache,
    value_cache,
    lengths,
    ffn_gain,
    routes,
    route_weight,
    expert_gate,
    expert_up,
    expert_down,
    dense_gate,
    dense_up,
    dense_down,
    gate_vector,
):
    seq_count, width = tokens.shape
    cache_len = key_cache.shape[1]
    devices = lax.axis_size("tp")
    experts_total = lax.axis_size("ep")
    slots = experts_total * CAP
    columns = width // devices
    keys = jnp.transpose(key_cache, (0, 2, 1, 3)).reshape(seq_count, cache_len, 2 * DQK)
    values = jnp.transpose(value_cache, (0, 2, 1, 3)).reshape(seq_count, cache_len, DV)
    partial = attend(
        lengths, lambdas, tokens, norm_gain[None], head_gain[None], query_weight, key_weight,
        value_weight, output_weight, keys, values,
    )
    parts = [partial] + [passed_on(partial, step) for step in range(1, devices)]
    (
        route_rows, weight_rows, near_tokens, near_gain, near_gate_vector,
        near_dense_gate, near_dense_up, near_dense_down,
    ) = load(
        partial, routes.T, route_weight.T, tokens, ffn_gain[None], gate_vector[None],
        dense_gate, dense_up, dense_down,
    )
    dispatch, mix = plan(route_rows, weight_rows, slots)
    residual, ffn_in, outbound = normalise(
        near_tokens, parts, near_gain, dispatch, columns
    )
    arrived = lax.all_to_all(outbound, "ep", split_axis=0, concat_axis=0, tiled=True)
    arrived, ffn_in = lax.optimization_barrier((arrived, ffn_in))
    gathered = [arrived] + [passed_on(arrived, step) for step in range(1, devices)]
    expert_weights, dense_blocks = dense_branch(
        ffn_in, near_dense_gate, near_dense_up, near_dense_down, near_gate_vector,
        (expert_gate[0], expert_up[0], expert_down[0]), devices,
    )
    dense_moved = [dense_blocks[0]]
    for step in range(1, devices):
        dense_moved.append(passed_on(dense_blocks[step], step))
    blocks = expert_rows(gathered, *expert_weights)
    moved = [blocks[0]] + [passed_on(blocks[step], step) for step in range(1, devices)]
    summed, kept = gather_parts(moved, dense_moved, residual, slots)
    returned = lax.all_to_all(summed, "ep", split_axis=0, concat_axis=0, tiled=True)
    return combine(kept, mix, returned)


def solution(mesh):
    placed = (
        P("ep", None),
        P(),
        P(None, "tp"),
        P(None, "tp"),
        P(None, "tp"),
        P("tp", None),
        P(),
        P("tp"),
        P("ep", None, "tp", None),
        P("ep", None, "tp", None),
        P("ep"),
        P(),
        P("ep", None),
        P("ep", None),
        P("ep", None, "tp"),
        P("ep", None, "tp"),
        P("ep", "tp", None),
        P("tp", None),
        P("tp", None),
        P("tp", None),
        P("tp"),
    )

    return jax.shard_map(
        shards, mesh=mesh, in_specs=placed, out_specs=P("ep", "tp"), check_vma=False
    )
```

```python
import jax
import jax.numpy as jnp
from jax import lax
from jax.experimental import pallas as pl
from jax.experimental.pallas import tpu as pltpu
from jax.sharding import PartitionSpec as P


DQK = 64
DV = 128
TOPK = 4
CAP = 2
GROUP = 8

epsilon = 1e-06
F32 = jnp.float32
BF16 = jnp.bfloat16


def rms_scale(values, gain):
    return values * lax.rsqrt(jnp.mean(values * values, axis=-1, keepdims=True) + epsilon) * gain


def dot(lhs, rhs, contract=((1,), (0,))):
    return lax.dot_general(lhs, rhs, (contract, ((), ())), preferred_element_type=F32)


def attention_kernel(
    lengths_hbm,
    lambdas_hbm,
    tokens_hbm,
    norm_gain_hbm,
    head_gain_hbm,
    query_hbm,
    key_hbm,
    value_hbm,
    output_hbm,
    key_cache,
    value_cache,
    partial_out,
    lengths,
    lambdas,
    tokens,
    norm_gain,
    head_gain,
    query_weight,
    key_weight,
    value_weight,
    output_weight,
    keys,
    values,
    mixture,
    sems,
):
    seq_count = tokens.shape[0]
    groups = seq_count // GROUP
    pairs = [
        (tokens_hbm, tokens),
        (norm_gain_hbm, norm_gain),
        (query_hbm, query_weight),
        (key_hbm, key_weight),
        (value_hbm, value_weight),
        (lengths_hbm, lengths),
        (lambdas_hbm, lambdas),
        (head_gain_hbm, head_gain),
    ]
    for group in range(groups):
        rows = pl.ds(group * GROUP, GROUP)
        pairs.append((key_cache.at[rows], keys.at[rows]))
        pairs.append((value_cache.at[rows], values.at[rows]))
    pairs.append((output_hbm, output_weight))
    copies = [
        pltpu.make_async_copy(source, target, sems.at[i])
        for i, (source, target) in enumerate(pairs)
    ]
    for copy in copies:
        copy.start()
    last = copies.pop()
    copies[0].wait()
    copies[1].wait()
    normed = rms_scale(tokens[...].astype(F32), norm_gain[...]).astype(BF16)
    copies[2].wait()
    queries = dot(normed, query_weight[...]).astype(BF16).astype(F32)
    copies[3].wait()
    new_keys = dot(normed, key_weight[...]).astype(BF16).astype(F32)
    copies[4].wait()
    new_values = dot(normed, value_weight[...]).astype(BF16).astype(F32)

    for copy in copies[5:8]:
        copy.wait()
    cache_len = keys.shape[1]
    row = lax.broadcasted_iota(jnp.int32, (8, 2 * DQK), 0)
    lane = lax.broadcasted_iota(jnp.int32, (8, 2 * DQK), 1)
    keep = jnp.logical_and((lane // DQK) == (row % 2), row < 4)
    row1 = lax.broadcasted_iota(jnp.int32, (8, 1), 0)
    sign = jnp.where(row1 % 2 == 0, 1.0, -jnp.where(row1 < 2, lambdas[0], lambdas[1]))
    position = lax.broadcasted_iota(jnp.int32, (8, cache_len), 1)
    score_scale = DQK ** (-0.5)
    for group in range(groups):
        copies[8 + 2 * group].wait()
        scores = []
        own_scores = []
        for s in range(group * GROUP, (group + 1) * GROUP):
            first = jnp.broadcast_to(queries[s : s + 1, : 2 * DQK], (8, 2 * DQK))
            second = jnp.broadcast_to(queries[s : s + 1, 2 * DQK :], (8, 2 * DQK))
            query = jnp.where(keep, jnp.where(row < 2, first, second), 0.0)
            score = dot(query.astype(BF16), keys[s], ((1,), (1,))) * score_scale
            scores.append(jnp.where(position < lengths[s], score, -jnp.inf))
            own_scores.append(
                jnp.sum(query * new_keys[s : s + 1, :], axis=1, keepdims=True) * score_scale
            )
        weights = []
        own_weights = []
        for score, own in zip(scores, own_scores):
            top = jnp.maximum(jnp.max(score, axis=1, keepdims=True), own)
            grown = jnp.exp(score - top)
            own_grown = jnp.exp(own - top)
            total = jnp.sum(grown, axis=1, keepdims=True) + own_grown
            share = sign / total
            prob = grown * share
            own_prob = own_grown * share
            weights.append((prob + pltpu.roll(prob, 7, 0)).astype(BF16))
            own_weights.append((own_prob + pltpu.roll(own_prob, 7, 0)).astype(BF16).astype(F32))
        copies[9 + 2 * group].wait()
        for i in range(GROUP):
            s = group * GROUP + i
            mixed = dot(weights[i], values[s]) + own_weights[i] * new_values[s : s + 1, :]
            mixture[s : s + 1, :DV] = mixed[0:1, :]
            mixture[s : s + 1, DV:] = mixed[2:3, :]
    gain = head_gain[...]
    left = rms_scale(mixture[:, :DV], gain).astype(BF16)
    right = rms_scale(mixture[:, DV:], gain).astype(BF16)
    last.wait()
    result = dot(left, output_weight[:DV, :]) + dot(right, output_weight[DV:, :])
    partial_out[...] = result.astype(BF16)


def whole(count):
    return [pl.BlockSpec(memory_space=pltpu.VMEM)] * count


def near(value):
    return pltpu.with_memory_space_constraint(value, pltpu.VMEM)


def all_far(*values):
    return [pltpu.with_memory_space_constraint(value, pltpu.HBM) for value in values]


def all_near(*values):
    return [near(value) for value in values]


def attend(lengths, lambdas, tokens, norm_gain, head_gain, query_weight, key_weight, value_weight,
           output_weight, key_cache, value_cache):
    seq_count, width = tokens.shape
    vectors = (tokens, norm_gain, head_gain, query_weight, key_weight, value_weight, output_weight,
               key_cache, value_cache)
    return pl.pallas_call(
        attention_kernel,
        name="attend",
        compiler_params=pltpu.CompilerParams(vmem_limit_bytes=16 << 20),
        out_shape=pltpu.VMEM((seq_count, width), BF16),
        in_specs=[pl.BlockSpec(memory_space=pltpu.HBM)] * 11,
        out_specs=whole(1)[0],
        scratch_shapes=[
            pltpu.SMEM(lengths.shape, lengths.dtype),
            pltpu.SMEM(lambdas.shape, lambdas.dtype),
            *[pltpu.VMEM(value.shape, value.dtype) for value in vectors],
            pltpu.VMEM((seq_count, 2 * DV), F32),
            pltpu.SemaphoreType.DMA((9 + 2 * (seq_count // GROUP),)),
        ],
    )(*all_far(lengths, lambdas, *vectors))


def slot_masks(routes, route_weight, slots):
    seq_count = routes.shape[1]
    slot_ids = lax.broadcasted_iota(jnp.int32, (slots, seq_count), 0)
    named = jnp.zeros((slots, seq_count), F32)
    weighed = jnp.zeros((slots, seq_count), F32)
    for k in range(TOPK):
        hit = (slot_ids // CAP) == routes[k : k + 1, :]
        named = named + jnp.where(hit, 1.0, 0.0)
        weighed = weighed + jnp.where(hit, route_weight[k : k + 1, :], 0.0)
    before = lax.broadcasted_iota(jnp.int32, (seq_count, seq_count), 0)
    after = lax.broadcasted_iota(jnp.int32, (seq_count, seq_count), 1)
    earlier = jnp.where(before < after, 1.0, 0.0).astype(BF16)
    rank = dot(named.astype(BF16), earlier)
    chosen = rank == (slot_ids % CAP).astype(F32)
    return jnp.where(chosen, named, 0.0), jnp.where(chosen, weighed, 0.0)


def three_pieces(values):
    high = values.astype(BF16)
    rest = values - high.astype(F32)
    middle = rest.astype(BF16)
    return high, middle, (rest - middle.astype(F32)).astype(BF16)


def load_kernel(after, routes_hbm, route_weight_hbm, *refs):
    count = (len(refs) - 5) // 2
    dispatch, mix = refs[count : count + 2]
    routes, route_weight, sems = refs[2 * count + 2 :]
    sources = (routes_hbm, route_weight_hbm, *refs[:count])
    targets = (routes, route_weight, *refs[count + 2 : 2 * count + 2])
    copies = [
        pltpu.make_async_copy(source, target, sems.at[i])
        for i, (source, target) in enumerate(zip(sources, targets))
    ]
    for copy in copies:
        copy.start()
    copies[0].wait()
    copies[1].wait()
    named, weighed = slot_masks(routes, route_weight, dispatch.shape[0])
    dispatch[...] = named.astype(BF16)
    for i, piece in enumerate(three_pieces(weighed.T)):
        mix[i] = piece
    for copy in copies[2:]:
        copy.wait()


def load(after, routes, route_weight, slots, *values):
    size = sum(value.size * value.dtype.itemsize for value in values)
    seq_count = routes.shape[1]
    outs = pl.pallas_call(
        load_kernel,
        name="load",
        compiler_params=pltpu.CompilerParams(vmem_limit_bytes=4 << 20),
        out_shape=(
            pltpu.VMEM((slots, seq_count), BF16),
            pltpu.VMEM((3, seq_count, slots), BF16),
            *[pltpu.VMEM(value.shape, value.dtype) for value in values],
        ),
        in_specs=whole(1) + [pl.BlockSpec(memory_space=pltpu.HBM)] * (2 + len(values)),
        out_specs=tuple(whole(2 + len(values))),
        scratch_shapes=[
            pltpu.VMEM(routes.shape, routes.dtype),
            pltpu.VMEM(route_weight.shape, route_weight.dtype),
            pltpu.SemaphoreType.DMA((2 + len(values),)),
        ],
        cost_estimate=pl.CostEstimate(
            flops=1 << 30, bytes_accessed=size, transcendentals=0
        ),
    )(near(after), *all_far(routes, route_weight, *values))
    return outs


def normalise_kernel(
    tokens, own, one, two, three, gain, dispatch, residual, ffn_in, outbound
):
    attention = (own[...].astype(F32) + one[...].astype(F32)) + (
        two[...].astype(F32) + three[...].astype(F32)
    )
    total = tokens[...].astype(F32) + attention
    residual[...] = total
    ffn_in[...] = rms_scale(total, gain[...]).astype(BF16)
    columns = outbound.shape[2]
    start = pl.multiple_of(lax.axis_index("tp") * columns, columns)
    sent = dot(dispatch[...], ffn_in[:, pl.ds(start, columns)]).astype(BF16)
    outbound[...] = sent.reshape(outbound.shape)


def normalise(tokens, parts, gain, dispatch, columns):
    seq_count, width = tokens.shape
    return pl.pallas_call(
        normalise_kernel,
        name="normalise",
        compiler_params=pltpu.CompilerParams(vmem_limit_bytes=8 << 20),
        out_shape=(
            pltpu.VMEM((seq_count, width), F32),
            pltpu.VMEM((seq_count, width), BF16),
            pltpu.VMEM((dispatch.shape[0] // CAP, CAP, columns), BF16),
        ),
        in_specs=whole(7),
        out_specs=tuple(whole(3)),
    )(*all_near(tokens, *parts, gain, dispatch))


def silu(values):
    return values / (1.0 + jnp.exp(-values))


def dense_kernel(rows, gate, up, down, vector, *refs):
    far, near_refs, blocks, sems = refs[:2], refs[2:4], refs[4:-1], refs[-1]
    copies = [
        pltpu.make_async_copy(source, target, sems.at[i])
        for i, (source, target) in enumerate(zip(far, near_refs))
    ]
    for copy in copies:
        copy.start()
    devices = len(blocks)
    seq_count, columns = rows.shape[0], blocks[0].shape[1]
    place = lax.axis_index("tp")
    value = rows[...]
    gate_pre = dot(value, gate[...], ((1,), (1,)))
    up_proj = dot(value, up[...], ((1,), (1,)))
    hidden = (silu(gate_pre) * up_proj).astype(BF16)
    part = jnp.sum(hidden.astype(F32) * vector[...], axis=1, keepdims=True)
    high, middle, low = three_pieces(part)
    lane = lax.broadcasted_iota(jnp.int32, (seq_count, columns), 1)
    pieces = jnp.where(
        lane == 0, high.astype(F32), jnp.where(lane == 1, middle.astype(F32), low.astype(F32))
    )
    logit = jnp.where(lane < 3, pieces, 0.0).astype(BF16)
    for step, block in enumerate(blocks):
        start = pl.multiple_of(((place + step) % devices) * columns, columns)
        block[:seq_count, :] = dot(hidden, down[:, pl.ds(start, columns)]).astype(BF16)
        block[seq_count:, :] = logit
    for copy in copies:
        copy.wait()


def dense_branch(rows, gate, up, down, vector, expert_weights, devices):
    seq_count, width = rows.shape
    block = pltpu.VMEM((2 * seq_count, width // devices), BF16)
    outs = pl.pallas_call(
        dense_kernel,
        name="dense",
        compiler_params=pltpu.CompilerParams(vmem_limit_bytes=8 << 20),
        out_shape=tuple(pltpu.VMEM(value.shape, value.dtype) for value in expert_weights)
        + (block,) * devices,
        in_specs=whole(5) + [pl.BlockSpec(memory_space=pltpu.HBM)] * 2,
        out_specs=tuple(whole(2 + devices)),
        scratch_shapes=[pltpu.SemaphoreType.DMA((2,))],
        cost_estimate=pl.CostEstimate(
            flops=6 * seq_count * width * gate.shape[0],
            bytes_accessed=6 * width * gate.shape[0],
            transcendentals=0,
        ),
    )(*all_near(rows, gate, up, down, vector), *all_far(*expert_weights))
    return outs[:2], outs[2:]


def expert_kernel(own, one, two, three, gate, up, down, *blocks):
    devices = len(blocks)
    place = lax.axis_index("tp")
    count, columns = own.shape[0] * own.shape[1], own.shape[2]
    gate_pre = jnp.zeros((count, gate.shape[1]), F32)
    up_proj = jnp.zeros((count, up.shape[1]), F32)
    for step, part in enumerate((own, one, two, three)):
        start = pl.multiple_of(((place + devices - step) % devices) * columns, columns)
        rows = part[...].reshape(count, columns)
        gate_pre = gate_pre + dot(rows, gate[pl.ds(start, columns), :])
        up_proj = up_proj + dot(rows, up[pl.ds(start, columns), :])
    hidden = (silu(gate_pre) * up_proj).astype(BF16)
    for step, block in enumerate(blocks):
        start = pl.multiple_of(((place + step) % devices) * columns, columns)
        block[...] = dot(hidden, down[:, pl.ds(start, columns)]).astype(BF16)


def expert_rows(parts, gate, up, down):
    devices = len(parts)
    experts, cap, columns = parts[0].shape
    return pl.pallas_call(
        expert_kernel,
        name="experts",
        compiler_params=pltpu.CompilerParams(vmem_limit_bytes=8 << 20),
        out_shape=(pltpu.VMEM((experts * cap, columns), BF16),) * devices,
        in_specs=whole(7),
        out_specs=tuple(whole(devices)),
    )(*all_near(*parts, gate, up, down))


def gather_kernel(own, one, two, three, dense_own, dense_one, dense_two, dense_three, residual,
                  summed, kept):
    columns = summed.shape[2]
    seq_count = residual.shape[0]
    total = (own[...].astype(F32) + one[...].astype(F32)) + (
        two[...].astype(F32) + three[...].astype(F32)
    )
    summed[...] = total.astype(BF16).reshape(summed.shape)
    dense = (dense_own[...].astype(F32) + dense_one[...].astype(F32)) + (
        dense_two[...].astype(F32) + dense_three[...].astype(F32)
    )
    pieces = dense[seq_count:, :]
    lane = lax.broadcasted_iota(jnp.int32, pieces.shape, 1)
    logit = jnp.sum(jnp.where(lane < 3, pieces, 0.0), axis=1, keepdims=True)
    gated = dense[:seq_count, :] / (1.0 + jnp.exp(-logit))
    start = pl.multiple_of(lax.axis_index("tp") * columns, columns)
    kept[...] = residual[:, pl.ds(start, columns)] + gated


def gather_parts(parts, dense_parts, residual, count):
    seq_count = residual.shape[0]
    columns = parts[0].shape[1]
    return pl.pallas_call(
        gather_kernel,
        name="gather",
        compiler_params=pltpu.CompilerParams(vmem_limit_bytes=8 << 20),
        out_shape=(
            pltpu.VMEM((count // CAP, CAP, columns), BF16),
            pltpu.VMEM((seq_count, columns), F32),
        ),
        in_specs=whole(9),
        out_specs=tuple(whole(2)),
    )(*all_near(*parts, *dense_parts, residual))


def combine_kernel(kept, mix, returned, out):
    rows = returned[...].reshape(mix.shape[2], -1)
    picked = dot(mix[0], rows) + (dot(mix[1], rows) + dot(mix[2], rows))
    out[...] = (kept[...] + picked).astype(BF16)


def combine(kept, mix, returned):
    return pl.pallas_call(
        combine_kernel,
        name="combine",
        compiler_params=pltpu.CompilerParams(vmem_limit_bytes=8 << 20),
        out_shape=jax.ShapeDtypeStruct(kept.shape, BF16),
        in_specs=whole(3),
        out_specs=whole(1)[0],
    )(*all_near(kept, mix, returned))


def passed_on(shard, step):
    devices = lax.axis_size("tp")
    return lax.ppermute(shard, "tp", [(i, (i + step) % devices) for i in range(devices)])


def shards(
    tokens,
    norm_gain,
    query_weight,
    key_weight,
    value_weight,
    output_weight,
    head_gain,
    lambdas,
    key_cache,
    value_cache,
    lengths,
    ffn_gain,
    routes,
    route_weight,
    expert_gate,
    expert_up,
    expert_down,
    dense_gate,
    dense_up,
    dense_down,
    gate_vector,
):
    seq_count, width = tokens.shape
    cache_len = key_cache.shape[1]
    devices = lax.axis_size("tp")
    experts_total = lax.axis_size("ep")
    slots = experts_total * CAP
    columns = width // devices
    keys = jnp.transpose(key_cache, (0, 2, 1, 3)).reshape(seq_count, cache_len, 2 * DQK)
    values = jnp.transpose(value_cache, (0, 2, 1, 3)).reshape(seq_count, cache_len, DV)
    partial = attend(
        lengths, lambdas, tokens, norm_gain[None], head_gain[None], query_weight, key_weight,
        value_weight, output_weight, keys, values,
    )
    parts = [partial] + [passed_on(partial, step) for step in range(1, devices)]
    (
        dispatch, mix, near_tokens, near_gain, near_gate_vector,
        near_dense_gate, near_dense_up, near_dense_down, near_expert_down,
    ) = load(
        partial, routes.T, route_weight.T, slots, tokens, ffn_gain[None], gate_vector[None],
        dense_gate, dense_up, dense_down, expert_down[0],
    )
    residual, ffn_in, outbound = normalise(
        near_tokens, parts, near_gain, dispatch, columns
    )
    arrived = lax.all_to_all(outbound, "ep", split_axis=0, concat_axis=0, tiled=True)
    arrived, ffn_in = lax.optimization_barrier((arrived, ffn_in))
    gathered = [arrived] + [passed_on(arrived, step) for step in range(1, devices)]
    expert_weights, dense_blocks = dense_branch(
        ffn_in, near_dense_gate, near_dense_up, near_dense_down, near_gate_vector,
        (expert_gate[0], expert_up[0]), devices,
    )
    dense_moved = [dense_blocks[0]]
    for step in range(1, devices):
        dense_moved.append(passed_on(dense_blocks[step], step))
    blocks = expert_rows(gathered, *expert_weights, near_expert_down)
    moved = [blocks[0]] + [passed_on(blocks[step], step) for step in range(1, devices)]
    summed, kept = gather_parts(moved, dense_moved, residual, slots)
    returned = lax.all_to_all(summed, "ep", split_axis=0, concat_axis=0, tiled=True)
    return combine(kept, mix, returned)


def solution(mesh):
    placed = (
        P("ep", None),
        P(),
        P(None, "tp"),
        P(None, "tp"),
        P(None, "tp"),
        P("tp", None),
        P(),
        P("tp"),
        P("ep", None, "tp", None),
        P("ep", None, "tp", None),
        P("ep"),
        P(),
        P("ep", None),
        P("ep", None),
        P("ep", None, "tp"),
        P("ep", None, "tp"),
        P("ep", "tp", None),
        P("tp", None),
        P("tp", None),
        P("tp", None),
        P("tp"),
    )

    return jax.shard_map(
        shards, mesh=mesh, in_specs=placed, out_specs=P("ep", "tp"), check_vma=False
    )
```
